256 devices in a mesh: dp: 4 (over x), kv: 32 (over z, y), tp: 2 (over core).
Axes of the slice: x: 4, y: 4, z: 8, core: 2. Of those that a mesh axis runs over, the one named last changes fastest.
Arguments:
- tokens: bfloat16 [4, 8192, 1024], P('dp', 'kv', 'tp'), may hold values from -6 to 6
- norm_gain: float32 [1024], replicated, may hold values from 0.1 to 1.9
- w_query: bfloat16 [1024, 1024], P(None, 'tp'), may hold values from -0.1875 to 0.1875
- w_key: bfloat16 [1024, 256], P(None, 'tp'), may hold values from -0.1875 to 0.1875
- w_value: bfloat16 [1024, 256], P(None, 'tp'), may hold values from -0.1875 to 0.1875
- q_gain: float32 [64], replicated, may hold values from 0.1 to 1.9
- k_gain: float32 [64], replicated, may hold values from 0.1 to 1.9
- w_out: bfloat16 [1024, 1024], P('tp'), may hold values from -4 to 4
- chosen: int32 [4, 256, 16], P('dp', 'kv'), may hold values from -1 to 255, as said below
Outputs:
- mixed: bfloat16 [4, 8192, 1024], P('dp', 'kv', 'tp')
- log_total: float32 [4, 16, 8192], P('dp', 'tp', 'kv')
The draws below stay inside these ranges and needn't reach their ends.
Inputs may be any that keep to these rules, and one draw needn't show every extreme that they name: Each row of chosen (one query block b) holds distinct key block numbers, all at most b, and -1 for empty entries; b itself is always present; a row is full (16 blocks) whenever at least 16 blocks may be chosen by it. Over the 8 rows of one index of kv, the chosen blocks that lie on any one other index of kv are at most 4 distinct ones, and exactly 4 of those on the index just before, for every index but the first. Some blocks are chosen far more often than others.
All inputs are finite; a program needn't handle non-finite values.
Results may differ from the reference program's by a relative error of at most 0.015.
Values may be sent and summed in bfloat16 or wider, within the bound.
A program may use at most 64 MiB of HBM per device.

```python
import jax
import jax.numpy as jnp
from jax import lax

D = 1024
H = 16
HD = 64
KVH = 4
BLK = 32
TOPB = 16
MOST = 4
NB_DEV = 8
NBLK = 256
SEQ = 8192
SEQS = 4
N_KV = 32


def chosen_sequence(seq_key):
    pop_key, cand_key, pick_key = jax.random.split(jax.random.fold_in(seq_key, 11), 3)
    block_ids = jnp.arange(NBLK, dtype=jnp.int32)
    owner_dev = block_ids // NB_DEV
    level_draw = jax.random.randint(pop_key, (NBLK,), 0, 4)
    appeal = level_draw * level_draw
    devices = jnp.arange(N_KV, dtype=jnp.int32)[:, None]
    noise_draw = jax.random.randint(cand_key, (N_KV, NBLK), 0, 1000)
    base_score = (appeal[None, :] * 1000 + noise_draw) * NBLK + block_ids[None, :]
    pinned = (block_ids[None, :] == devices * NB_DEV - 1) | (block_ids[None, :] == (devices - N_KV // 2) * NB_DEV)
    priority = jnp.where(pinned, base_score + 268435456, base_score).reshape(N_KV, N_KV, NB_DEV)
    threshold_val = lax.top_k(priority, MOST)[0][..., -1:]
    kept_set = (priority >= threshold_val).reshape(N_KV, NBLK)
    kept_set = jnp.where(owner_dev[None, :] == devices, True, kept_set & (owner_dev[None, :] < devices))
    query_ids = block_ids[:, None]
    row_dev = query_ids // NB_DEV
    candidate = kept_set[row_dev[:, 0]]
    allowed = candidate & (block_ids[None, :] <= query_ids)
    local_pos = query_ids % NB_DEV
    forced = (block_ids[None, :] == query_ids) | (block_ids[None, :] == query_ids - 1)
    forced = forced | (local_pos == 0) & (block_ids[None, :] == (row_dev - N_KV // 2) * NB_DEV)
    forced = forced | (local_pos == NB_DEV - 1) & candidate & (owner_dev[None, :] == row_dev - 1)
    second_noise = jax.random.randint(pick_key, (NBLK, NBLK), 0, 1000)
    ranking = (appeal[None, :] * 1000 + second_noise) * NBLK + block_ids[None, :]
    ranking = jnp.where(forced, ranking + 268435456, ranking)
    ranking = jnp.where(allowed, ranking, -1 - block_ids[None, :])
    top_vals, top_ids = lax.top_k(ranking, TOPB)
    return jnp.where(top_vals >= 0, top_ids, -1).astype(jnp.int32)


def draw_chosen(key, part):
    seq_keys = jax.random.split(jax.random.fold_in(key, 5), SEQS)
    return jax.vmap(chosen_sequence)(seq_keys)


def block_scale(key, dims, cuts, least, largest):
    factor_of = 1.0
    for position, parts in cuts:
        steps = jax.random.uniform(jax.random.fold_in(jax.random.fold_in(key, 6), position), (parts,), jnp.float32, least / len(cuts), largest / len(cuts))
        factor_of = factor_of * jnp.repeat(jnp.exp(steps), dims[position] // parts).reshape((-1,) + (1,) * (len(dims) - 1 - position))
    return factor_of


def gaussian(rng, extent, scale, bound, cuts=(), kind=jnp.bfloat16):
    entries = jax.random.normal(rng, extent, jnp.float32) * scale
    if len(cuts) > 0:
        entries = block_scale(rng, extent, cuts, -0.22, 0.18) * entries
    return jnp.clip(entries, min=-bound, max=bound).astype(kind)


def setup_inputs(seed: int = 0) -> dict:
    key_of = jax.random.split(jax.random.key(seed), 10)
    return {
        "tokens": gaussian(key_of[0], (SEQS, SEQ, D), 1.0, 6.0, ((0, 4), (1, 32), (2, 2))),
        "norm_gain": jnp.clip(1.0 + 0.18 * jax.random.normal(key_of[1], (D,), jnp.float32), 0.1, 1.9),
        "w_query": gaussian(key_of[2], (D, H * HD), D ** -0.5, 0.1875, ((1, 2),)),
        "w_key": gaussian(key_of[3], (D, KVH * HD), D ** -0.5, 0.1875, ((1, 2),)),
        "w_value": gaussian(key_of[4], (D, KVH * HD), D ** -0.5, 0.1875, ((1, 2),)),
        "q_gain": jnp.clip(1.0 + 0.18 * jax.random.normal(key_of[5], (HD,), jnp.float32), 0.1, 1.9),
        "k_gain": jnp.clip(1.0 + 0.18 * jax.random.normal(key_of[6], (HD,), jnp.float32), 0.1, 1.9),
        "w_out": gaussian(key_of[7], (H * HD, D), (8 * (H * HD) ** -0.5), 4.0, ((0, 2),)),
        "chosen": draw_chosen(jax.random.fold_in(key_of[9], 71), 0),
    }


epsilon = 1e-06
alibi_reach = 4.0

def rms_norm(values, gain):
    return values * lax.rsqrt(lax.optimization_barrier(jnp.mean(values * values, axis=-1, keepdims=True)) + epsilon) * gain.astype(jnp.float32)

def reference(tokens, norm_gain, w_query, w_key, w_value, q_gain, k_gain, w_out, chosen):
    group_size = H // KVH
    slopes = jnp.exp2(-8.0 * jnp.arange(1, H + 1, dtype=jnp.float32) / H)

    def one_sequence(seq_args):
        sequence_tokens, sequence_chosen = seq_args
        hidden = rms_norm(sequence_tokens.astype(jnp.float32), norm_gain).astype(jnp.bfloat16)
        queries = rms_norm(jnp.dot(hidden, w_query, preferred_element_type=jnp.float32).reshape(SEQ, H, HD), q_gain).astype(jnp.bfloat16)
        key_rows = rms_norm(jnp.dot(hidden, w_key, preferred_element_type=jnp.float32).reshape(SEQ, KVH, HD), k_gain).astype(jnp.bfloat16)
        value_rows = jnp.dot(hidden, w_value, preferred_element_type=jnp.float32).astype(jnp.bfloat16).reshape(SEQ, KVH, HD)
        key_blocks = key_rows.reshape(NBLK, BLK, KVH, HD)
        value_blocks = value_rows.reshape(NBLK, BLK, KVH, HD)

        def one_block(block_args):
            block_index, requested, query_block = block_args
            present = requested >= 0
            clamped = jnp.maximum(requested, 0).astype(jnp.int32)
            picked_keys = jnp.repeat(key_blocks[clamped].reshape(TOPB * BLK, KVH, HD), group_size, axis=1)
            picked_values = jnp.repeat(value_blocks[clamped].reshape(TOPB * BLK, KVH, HD), group_size, axis=1)
            scores = jnp.einsum('qhd,khd->hqk', query_block.astype(jnp.float32), picked_keys.astype(jnp.float32), precision=lax.Precision.HIGHEST) * HD ** (-0.5)
            query_pos = block_index * BLK + jnp.arange(BLK, dtype=jnp.int32)
            key_pos = (clamped[:, None] * BLK + jnp.arange(BLK, dtype=jnp.int32)[None, :]).reshape(-1)
            offset = (query_pos[:, None] - key_pos[None, :]).astype(jnp.float32)
            scores = scores - slopes[:, None, None] * offset[None] * alibi_reach / SEQ
            allowed = jnp.repeat(present, BLK)[None, :] & (offset >= 0)
            scores = jnp.where(allowed[None], scores, -jnp.inf)
            row_max = lax.optimization_barrier(jnp.max(scores, axis=-1, keepdims=True))
            weights = jnp.exp(scores - row_max)
            row_sum = lax.optimization_barrier(jnp.sum(weights, axis=-1, keepdims=True))
            block_log = row_max[..., 0] + jnp.log(row_sum[..., 0])
            probs = lax.optimization_barrier((weights / row_sum).astype(jnp.bfloat16))
            block_out = jnp.einsum('hqk,khd->qhd', probs.astype(jnp.float32), picked_values.astype(jnp.float32), precision=lax.Precision.HIGHEST)
            return (block_out, block_log)
        block_ids = jnp.arange(NBLK, dtype=jnp.int32)
        block_out, block_log = lax.map(one_block, (block_ids, sequence_chosen, queries.reshape(NBLK, BLK, H, HD)))
        attended = block_out.reshape(SEQ, H * HD).astype(jnp.bfloat16)
        mixed = jnp.dot(attended, w_out, preferred_element_type=jnp.float32).astype(jnp.bfloat16)
        log_total = block_log.transpose(1, 0, 2).reshape(H, SEQ)
        return (mixed, log_total)
    mixed, log_total = lax.map(one_sequence, (tokens, chosen))
    return (mixed, log_total)
```

```python
import functools
import math

import jax
import jax.numpy as jnp
from jax import lax
from jax.experimental import pallas as pl
from jax.experimental.pallas import tpu as pltpu
from jax.sharding import PartitionSpec as P

MESH = pl.DeviceIdType.MESH
F32 = jnp.float32
BF16 = jnp.bfloat16
I32 = jnp.int32

NZ, NY = 8, 4
NB = 8
BLK = 32
TOPB = 16
MOST = 4
HD = 64
HEADS = 8
TOK = NB * BLK
EPS = 1e-6
SEQ = 8192
OWN = NZ * NY * MOST
LANDED = OWN + NB
FAR = -1e30
PAIRS = ((0, 5), (2, 7), (1, 4), (3, 6))
LOG2E = math.log2(math.e)


def half_sums(x):
    row = lax.broadcasted_iota(I32, (128, 128), 0) // HD
    col = lax.broadcasted_iota(I32, (128, 128), 1) // HD
    ones = jnp.where(row == col, 1.0, 0.0).astype(BF16)
    high = x.astype(BF16)
    low = (x - high.astype(F32)).astype(BF16)
    return jnp.dot(high, ones, preferred_element_type=F32) + jnp.dot(
        low, ones, preferred_element_type=F32
    )


def head_norm(x, gain):
    return x * lax.rsqrt(half_sums(x * x) * (1.0 / HD) + EPS) * gain


def kernel(
    tokens, gain, wq, wk, wv, qg, kg, wo, chosen,
    out, logs,
    tok, hid, wq_v, wkv_v, wo_v,
    c0, c1, c2, c3, c4, c5, c6, c7,
    msg, land, sel_v, nsel_v, ent_v, sel_s, nsel_s, ent_s,
    upos, bias_t, bias_a, qbd, kvg, att, lsum, part, part_in,
    load_sem, tab_sem, tok_send, tok_recv, nsel_send, nsel_recv,
    up_send, up_recv, dn_send, dn_recv, y_send, y_recv, out_send, out_recv,
):
    dp = lax.axis_index("dp")
    kv = lax.axis_index("kv")
    tp = lax.axis_index("tp")
    z = kv // NY
    y = kv % NY
    col = (c0, c1, c2, c3, c4, c5, c6, c7)

    def dev(dz, dy):
        return (dp, ((z + dz) % NZ) * NY + (y + dy) % NY, tp)

    partner = (dp, kv, 1 - tp)

    def remote(src, dst, send, recv, where):
        return pltpu.make_async_remote_copy(
            src_ref=src, dst_ref=dst, send_sem=send, recv_sem=recv,
            device_id=where, device_id_type=MESH,
        )

    loads = [
        pltpu.make_async_copy(tokens, tok.at[tp], load_sem.at[0]),
        pltpu.make_async_copy(wk, wkv_v.at[:, pl.ds(0, 128)], load_sem.at[1]),
        pltpu.make_async_copy(wv, wkv_v.at[:, pl.ds(128, 128)], load_sem.at[2]),
        pltpu.make_async_copy(wq, wq_v, load_sem.at[3]),
    ]
    for p, pair in enumerate(PAIRS):
        for side in range(2):
            loads.append(
                pltpu.make_async_copy(
                    wo.at[pl.ds(pair[side] * HD, HD), :],
                    wo_v.at[pl.ds(p * 128 + side * HD, HD), :],
                    load_sem.at[4 + 2 * p + side],
                )
            )
    for load in loads:
        load.start()

    barrier = pltpu.get_barrier_semaphore()
    peers = [partner, dev(0, 1), dev(0, 2), dev(0, 3), dev(1, 0), dev(-1, 0)]
    for peer in peers:
        pl.semaphore_signal(barrier, inc=1, device_id=peer, device_id_type=MESH)
    pl.semaphore_wait(barrier, len(peers))

    tok_copy = remote(tokens, tok.at[tp], tok_send.at[0], tok_recv.at[0], partner)
    tok_copy.start()

    ch = chosen[...]
    lane = lax.broadcasted_iota(I32, (NB, 256), 1)
    own_block = kv * NB + lax.broadcasted_iota(I32, (NB, 1), 0)
    member = jnp.zeros((NB, 256), I32)
    for e in range(TOPB):
        member = jnp.where(ch[:, e : e + 1] == lane, 1, member)
    present = jnp.broadcast_to(jnp.max(member, axis=0, keepdims=True), (NB, 256))
    inner = lane % NB
    rank = jnp.zeros((NB, 256), I32)
    for k in range(1, NB):
        rank = rank + jnp.where(inner >= k, pltpu.roll(present, k, 1), 0)
    sub = lax.broadcasted_iota(I32, (NB, 256), 0)
    sel = jnp.zeros((NB, 256), I32)
    for s in range(MOST):
        val = jnp.where((present == 1) & (rank == s), inner, 0)
        for k in (1, 2, 4):
            val = val + pltpu.roll(val, 256 - k, 1)
        sel = jnp.where(sub == s, val, sel)
    sel_v[...] = sel
    chip = lane // NB
    from_y = (y - chip % NY + NY) % NY
    from_z = (z - chip // NY + NZ) % NZ
    spot_of = jnp.where(
        chip == kv,
        OWN + inner,
        (from_y * NZ + from_z) * MOST + rank,
    )
    front = jnp.where(
        lax.broadcasted_iota(I32, (NB, TOPB), 1) == 0,
        own_block,
        jnp.where(ch == own_block, ch[:, 0:1], ch),
    )
    filled = jnp.where(front < 0, own_block, front)
    lane_e = lax.broadcasted_iota(I32, (NB, 128), 1)
    entry = jnp.zeros((NB, 128), I32)
    lane_u = lax.broadcasted_iota(I32, (NB, TOPB * BLK), 1)
    pos = jnp.full((NB, TOPB * BLK), FAR, F32)
    for e in range(TOPB):
        at = jnp.sum(jnp.where(filled[:, e : e + 1] == lane, spot_of, 0), axis=1, keepdims=True)
        entry = jnp.where(lane_e == e, at, entry)
        first = front[:, e : e + 1]
        pos = jnp.where(
            (lane_u // BLK == e) & (first >= 0),
            (first * BLK + lane_u % BLK).astype(F32),
            pos,
        )
    ent_v[...] = entry
    for r in range(NB):
        upos[r] = jnp.broadcast_to(pos[r : r + 1], (8, TOPB * BLK))

    nsel_copies = []
    for dy in range(1, NY):
        c = remote(sel_v, nsel_v.at[dy], nsel_send.at[dy], nsel_recv.at[dy], dev(0, dy))
        c.start()
        nsel_copies.append(c)
    tabs = [
        pltpu.make_async_copy(sel_v, sel_s, tab_sem.at[0]),
        pltpu.make_async_copy(ent_v, ent_s, tab_sem.at[1]),
    ]
    for t in tabs:
        t.start()

    rows = lax.broadcasted_iota(I32, (TOK, 128), 0)
    head_no = (tp * HEADS + rows // BLK + 1).astype(F32)
    bias_t[...] = (rows % BLK).astype(F32)
    bias_a[...] = jnp.exp2(head_no * (-8.0 / 16.0)) * (4.0 / SEQ * LOG2E)
    lsum[...] = jnp.zeros((TOK, 256), F32)

    loads[0].wait()
    tok_copy.wait_recv()
    g0 = gain[:, 0:512]
    g1 = gain[:, 512:1024]

    def norm_rows(i, carry):
        at = pl.ds(i * 32, 32)
        a = tok[0, at, :].astype(F32)
        b = tok[1, at, :].astype(F32)
        total = jnp.sum(a * a + b * b, axis=1, keepdims=True)
        r = lax.rsqrt(total * (1.0 / 1024.0) + EPS)
        hid[at, 0:512] = (a * r * g0).astype(BF16)
        hid[at, 512:1024] = (b * r * g1).astype(BF16)
        return carry

    lax.fori_loop(0, 8, norm_rows, 0)
    loads[1].wait()
    loads[2].wait()
    kgain = jnp.concatenate([kg[...], kg[...]], axis=1)
    qgain = jnp.concatenate([qg[...], qg[...]], axis=1)
    both = jnp.dot(hid[...], wkv_v[...], preferred_element_type=F32)
    keys = head_norm(both[:, 0:128], kgain).astype(BF16)
    values = both[:, 128:256].astype(BF16)
    for k, rows_of in enumerate((keys, values)):
        blocks = rows_of.reshape(NB, BLK, 128)
        c0[:, :, 128 * k : 128 * (k + 1)] = blocks
        land[pl.ds(OWN, NB), :, 128 * k : 128 * (k + 1)] = blocks

    def up(d, half):
        at = pl.ds(half * 4, 4)
        return remote(
            col[d].at[at], col[d + 1].at[at],
            up_send.at[2 * d + half], up_recv.at[2 * d + half], dev(1, 0),
        )

    def down(d, half):
        at = pl.ds(half * 4, 4)
        return remote(
            col[(8 - d) % 8].at[at], col[7 - d].at[at],
            dn_send.at[2 * d + half], dn_recv.at[2 * d + half], dev(-1, 0),
        )

    ups = [[up(d, half) for half in range(2)] for d in range(4)]
    downs = [[down(d, half) for half in range(2)] for d in range(3)]
    for half in range(2):
        ups[0][half].start()
        downs[0][half].start()

    y_copies = {}

    def pick(d, dy):
        source = (((z - d + NZ) % NZ) * NY + y) * NB
        for s in range(MOST):
            which = sel_s[s, source] if dy == 0 else nsel_s[dy, s, source]
            block = col[d][which]
            if dy == 0:
                land[d * MOST + s] = block
            else:
                msg[dy * NZ + d, s] = block

    def serve(d):
        for dy in range(1, NY):
            pick(d, dy)
        for dy in range(1, NY):
            k = dy * NZ + d
            c = remote(
                msg.at[k], land.at[pl.ds(k * MOST, MOST)],
                y_send.at[k], y_recv.at[k], dev(0, dy),
            )
            c.start()
            y_copies[k] = c
        if d:
            pick(d, 0)

    for c in nsel_copies:
        c.wait_recv()
    ntab = [
        pltpu.make_async_copy(nsel_v.at[NY - dy], nsel_s.at[dy], tab_sem.at[1 + dy])
        for dy in range(1, NY)
    ]
    for t in ntab:
        t.start()
    for t in tabs + ntab:
        t.wait()
    serve(0)

    loads[3].wait()
    flat = jnp.dot(hid[...], wq_v[...], preferred_element_type=F32)
    normed = [head_norm(flat[:, 128 * t : 128 * (t + 1)], qgain) for t in range(4)]
    low_half = lax.broadcasted_iota(I32, (TOK, 128), 1) < HD
    turned = [pltpu.roll(x, HD, 1) for x in normed]
    paired = (
        jnp.where(low_half, normed[0], normed[2]),
        jnp.where(low_half, normed[1], normed[3]),
        jnp.where(low_half, turned[0], turned[2]),
        jnp.where(low_half, turned[1], turned[3]),
    )
    for p, pair in enumerate(PAIRS):
        first = jnp.where(low_half, paired[p], 0.0).astype(BF16)
        second = jnp.where(low_half, 0.0, paired[p]).astype(BF16)
        for r in range(NB):
            qbd[r, pl.ds(pair[0] * BLK, BLK), :] = first[r * BLK : (r + 1) * BLK]
            qbd[r, pl.ds(pair[1] * BLK, BLK), :] = second[r * BLK : (r + 1) * BLK]

    for k in range(1, 5):
        for half in range(2):
            ups[k - 1][half].wait_recv()
            if k < 4:
                ups[k][half].start()
            if k < 4:
                downs[k - 1][half].wait_recv()
                if k < 3:
                    downs[k][half].start()
        serve(k)
        if k < 4:
            serve(8 - k)
    for load in loads[4:]:
        load.wait()
    for c in y_copies.values():
        c.wait_recv()

    def attend(r, carry):
        for e in range(TOPB):
            kvg[pl.ds(e * BLK, BLK), :] = land[ent_s[r, e]]
        raw = lax.dot_general(
            qbd[r], kvg[:, 0:128], (((1,), (1,)), ((), ())), preferred_element_type=F32
        )
        t = bias_t[...] + ((kv * NB + r) * BLK).astype(F32)
        a = bias_a[...]
        total = jnp.zeros((TOK, 128), F32)
        probs = []
        for i in range(4):
            u = upos[r, 0:1, 128 * i : 128 * (i + 1)]
            if i == 0:
                off = jnp.where(u > t, FAR, u - t)
            else:
                off = u - t
            w = jnp.exp2(raw[:, 128 * i : 128 * (i + 1)] * (LOG2E / 8.0) + a * off)
            total = total + w
            probs.append(w.astype(BF16))
        row_sum = jnp.sum(total, axis=1, keepdims=True)
        weighted = jnp.dot(
            jnp.concatenate(probs, axis=1), kvg[:, 128:256], preferred_element_type=F32
        )
        weighted = weighted / row_sum
        low = lax.broadcasted_iota(I32, (BLK, 128), 1) < HD
        for p, pair in enumerate(PAIRS):
            tile = jnp.where(
                low,
                weighted[pair[0] * BLK : (pair[0] + 1) * BLK],
                weighted[pair[1] * BLK : (pair[1] + 1) * BLK],
            )
            att[pl.ds(pl.multiple_of(r * BLK, BLK), BLK), 128 * p : 128 * (p + 1)] = tile.astype(
                BF16
            )
        spot = lax.broadcasted_iota(I32, (TOK, 256), 1)
        query = lax.broadcasted_iota(I32, (TOK, 256), 0) % BLK
        lsum[...] = jnp.where(spot == r * BLK + query, row_sum, lsum[...])
        return carry

    out_copies = []
    for piece in range(2):
        lax.fori_loop(piece * 4, piece * 4 + 4, attend, 0)
        at = pl.ds(piece * 128, 128)
        rows_in = att[at, :]
        theirs = pl.multiple_of((1 - tp) * 512, 512)
        part[at, :] = jnp.dot(
            rows_in, wo_v[:, pl.ds(theirs, 512)], preferred_element_type=F32
        ).astype(BF16)
        c = remote(
            part.at[at, :], part_in.at[at, :], out_send.at[piece], out_recv.at[piece], partner
        )
        c.start()
        out_copies.append(c)
    logs[...] = jnp.log(jnp.sum(lsum[...].reshape(HEADS, BLK, 256), axis=1))
    mine = pl.multiple_of(tp * 512, 512)
    for piece in range(2):
        at = pl.ds(piece * 128, 128)
        own = jnp.dot(att[at, :], wo_v[:, pl.ds(mine, 512)], preferred_element_type=F32)
        out_copies[piece].wait_recv()
        out[at, :] = (own + part_in[at, :].astype(F32)).astype(BF16)

    tok_copy.wait_send()
    for c in nsel_copies + out_copies + list(y_copies.values()):
        c.wait_send()
    for pair in ups + downs:
        for c in pair:
            c.wait_send()


def body(tokens, norm_gain, w_query, w_key, w_value, q_gain, k_gain, w_out, chosen):
    any_space = pl.BlockSpec(memory_space=pl.ANY)
    vmem = pl.BlockSpec(memory_space=pltpu.VMEM)
    dma = pltpu.SemaphoreType.DMA
    mixed, logs = pl.pallas_call(
        kernel,
        out_shape=(
            jax.ShapeDtypeStruct((TOK, 512), BF16),
            jax.ShapeDtypeStruct((HEADS, TOK), F32),
        ),
        in_specs=[any_space, vmem, any_space, any_space, any_space, vmem, vmem, any_space, vmem],
        out_specs=(vmem, vmem),
        scratch_shapes=[
            pltpu.VMEM((2, TOK, 512), BF16),
            pltpu.VMEM((TOK, 1024), BF16),
            pltpu.VMEM((1024, 512), BF16),
            pltpu.VMEM((1024, 256), BF16),
            pltpu.VMEM((512, 1024), BF16),
            *[pltpu.VMEM((NB, BLK, 256), BF16) for _ in range(8)],
            pltpu.VMEM((NZ * NY, MOST, BLK, 256), BF16),
            pltpu.VMEM((LANDED, BLK, 256), BF16),
            pltpu.VMEM((NB, 256), I32),
            pltpu.VMEM((NY, NB, 256), I32),
            pltpu.VMEM((NB, 128), I32),
            pltpu.SMEM((NB, 256), I32),
            pltpu.SMEM((NY, NB, 256), I32),
            pltpu.SMEM((NB, 128), I32),
            pltpu.VMEM((NB, 8, TOPB * BLK), F32),
            pltpu.VMEM((TOK, 128), F32),
            pltpu.VMEM((TOK, 128), F32),
            pltpu.VMEM((NB, TOK, 128), BF16),
            pltpu.VMEM((TOPB * BLK, 256), BF16),
            pltpu.VMEM((TOK, 512), BF16),
            pltpu.VMEM((TOK, 256), F32),
            pltpu.VMEM((TOK, 512), BF16),
            pltpu.VMEM((TOK, 512), BF16),
            dma((12,)),
            dma((5,)),
            dma((1,)), dma((1,)),
            dma((NY,)), dma((NY,)),
            dma((8,)), dma((8,)),
            dma((6,)), dma((6,)),
            dma((NZ * NY,)), dma((NZ * NY,)),
            dma((2,)), dma((2,)),
        ],
        compiler_params=pltpu.CompilerParams(
            collective_id=0, has_side_effects=True, vmem_limit_bytes=48 * 1024 * 1024
        ),
        name="fused",
    )(
        tokens.reshape(TOK, 512),
        norm_gain.reshape(1, 1024),
        w_query,
        w_key,
        w_value,
        q_gain.reshape(1, HD),
        k_gain.reshape(1, HD),
        w_out,
        chosen.reshape(NB, TOPB),
    )
    return mixed.reshape(1, TOK, 512), logs.reshape(1, HEADS, TOK)


def solution(mesh):
    return jax.shard_map(
        body,
        mesh=mesh,
        in_specs=(
            P("dp", "kv", "tp"), P(), P(None, "tp"), P(None, "tp"), P(None, "tp"),
            P(), P(), P("tp", None), P("dp", "kv", None),
        ),
        out_specs=(P("dp", "kv", "tp"), P("dp", "tp", "kv")),
        check_vma=False,
    )
```

```python
import functools
import math

import jax
import jax.numpy as jnp
from jax import lax
from jax.experimental import pallas as pl
from jax.experimental.pallas import tpu as pltpu
from jax.sharding import PartitionSpec as P

MESH = pl.DeviceIdType.MESH
F32 = jnp.float32
BF16 = jnp.bfloat16
I32 = jnp.int32

NZ, NY = 8, 4
NB = 8
BLK = 32
TOPB = 16
MOST = 4
HD = 64
HEADS = 8
TOK = NB * BLK
EPS = 1e-6
SEQ = 8192
OWN = NZ * NY * MOST
LANDED = OWN + NB
FAR = -1e30
PAIRS = ((0, 5), (2, 7), (1, 4), (3, 6))
NEAR = ((0, 1), (0, 2), (0, 3), (1, 0), (-1, 0), (2, 0), (-2, 0))
SERVED = ((0, 1), (0, 2), (0, 3), (2, 0), (-2, 0), (-1, 0))
CHUNKS = 4
PIECES = 4
PER = NB // PIECES
LOG2E = math.log2(math.e)


def half_sums(x):
    row = lax.broadcasted_iota(I32, (128, 128), 0) // HD
    col = lax.broadcasted_iota(I32, (128, 128), 1) // HD
    ones = jnp.where(row == col, 1.0, 0.0).astype(BF16)
    high = x.astype(BF16)
    low = (x - high.astype(F32)).astype(BF16)
    return jnp.dot(high, ones, preferred_element_type=F32) + jnp.dot(
        low, ones, preferred_element_type=F32
    )


def head_norm(x, gain):
    return x * lax.rsqrt(half_sums(x * x) * (1.0 / HD) + EPS) * gain


def kernel(
    tokens, gain_h, wq, wk, wv, qg_h, kg_h, wo, chosen_h,
    out, logs,
    chosen, gain, qg, kg, tok, hid, wq_v, wkv_v, wo_v,
    c0, c1, c2, c3, c4, c5, c6, c7, p1, p2, p3,
    msg, land, sel_v, nsel_v, ent_v, sel_s, nsel_s, ent_s,
    upos, bias_t, bias_a, qbd, kvg, att, lsum, part, part_in,
    small_sem, load_sem, tab_sem, tok_send, tok_recv, nsel_send, nsel_recv,
    up_send, up_recv, dn_send, dn_recv, pln_send, pln_recv, y_send, y_recv, out_send, out_recv,
):
    dp = lax.axis_index("dp")
    kv = lax.axis_index("kv")
    tp = lax.axis_index("tp")
    z = kv // NY
    y = kv % NY
    col = (c0, c1, c2, c3, c4, c5, c6, c7)
    plane = (c0, p1, p2, p3)

    def dev(dz, dy):
        return (dp, ((z + dz) % NZ) * NY + (y + dy) % NY, tp)

    partner = (dp, kv, 1 - tp)

    def remote(src, dst, send, recv, where):
        return pltpu.make_async_remote_copy(
            src_ref=src, dst_ref=dst, send_sem=send, recv_sem=recv,
            device_id=where, device_id_type=MESH,
        )

    barrier = pltpu.get_barrier_semaphore()
    peers = [partner] + [dev(*at) for at in NEAR]
    for peer in peers:
        pl.semaphore_signal(barrier, inc=1, device_id=peer, device_id_type=MESH)

    small = [
        pltpu.make_async_copy(src, dst, small_sem.at[n])
        for n, (src, dst) in enumerate(
            ((chosen_h, chosen), (gain_h, gain), (qg_h, qg), (kg_h, kg))
        )
    ]
    for load in small:
        load.start()
    loads = [
        pltpu.make_async_copy(tokens, tok.at[tp], load_sem.at[0]),
        pltpu.make_async_copy(wk, wkv_v.at[:, pl.ds(0, 128)], load_sem.at[1]),
        pltpu.make_async_copy(wv, wkv_v.at[:, pl.ds(128, 128)], load_sem.at[2]),
        pltpu.make_async_copy(wq, wq_v, load_sem.at[3]),
    ]
    for p, pair in enumerate(PAIRS):
        for side in range(2):
            loads.append(
                pltpu.make_async_copy(
                    wo.at[pl.ds(pair[side] * HD, HD), :],
                    wo_v.at[pl.ds(p * 128 + side * HD, HD), :],
                    load_sem.at[4 + 2 * p + side],
                )
            )
    for load in loads:
        load.start()

    small[0].wait()
    ch = chosen[...]
    lane = lax.broadcasted_iota(I32, (NB, 256), 1)
    own_block = kv * NB + lax.broadcasted_iota(I32, (NB, 1), 0)
    member = jnp.zeros((NB, 256), I32)
    for e in range(TOPB):
        member = jnp.where(ch[:, e : e + 1] == lane, 1, member)
    present = jnp.broadcast_to(jnp.max(member, axis=0, keepdims=True), (NB, 256))
    inner = lane % NB
    rank = jnp.zeros((NB, 256), I32)
    for k in range(1, NB):
        rank = rank + jnp.where(inner >= k, pltpu.roll(present, k, 1), 0)
    sub = lax.broadcasted_iota(I32, (NB, 256), 0)
    sel = jnp.zeros((NB, 256), I32)
    for s in range(MOST):
        val = jnp.where((present == 1) & (rank == s), inner, 0)
        for k in (1, 2, 4):
            val = val + pltpu.roll(val, 256 - k, 1)
        sel = jnp.where(sub == s, val, sel)
    sel_v[...] = sel
    chip = lane // NB
    from_y = (y - chip % NY + NY) % NY
    from_z = (z - chip // NY + NZ) % NZ
    spot_of = jnp.where(
        chip == kv,
        OWN + inner,
        (from_y * NZ + from_z) * MOST + rank,
    )
    front = jnp.where(
        lax.broadcasted_iota(I32, (NB, TOPB), 1) == 0,
        own_block,
        jnp.where(ch == own_block, ch[:, 0:1], ch),
    )
    filled = jnp.where(front < 0, own_block, front)
    lane_e = lax.broadcasted_iota(I32, (NB, 128), 1)
    entry = jnp.zeros((NB, 128), I32)
    lane_u = lax.broadcasted_iota(I32, (NB, TOPB * BLK), 1)
    pos = jnp.full((NB, TOPB * BLK), FAR, F32)
    for e in range(TOPB):
        at = jnp.sum(jnp.where(filled[:, e : e + 1] == lane, spot_of, 0), axis=1, keepdims=True)
        entry = jnp.where(lane_e == e, at, entry)
        first = front[:, e : e + 1]
        pos = jnp.where(
            (lane_u // BLK == e) & (first >= 0),
            (first * BLK + lane_u % BLK).astype(F32),
            pos,
        )
    ent_v[...] = entry
    for r in range(NB):
        upos[r] = jnp.broadcast_to(pos[r : r + 1], (8, TOPB * BLK))

    rows = lax.broadcasted_iota(I32, (TOK, 128), 0)
    head_no = (tp * HEADS + rows // BLK + 1).astype(F32)
    bias_t[...] = (rows % BLK).astype(F32)
    bias_a[...] = jnp.exp2(head_no * (-8.0 / 16.0)) * (4.0 / SEQ * LOG2E)
    lsum[...] = jnp.zeros((TOK, 256), F32)

    pl.semaphore_wait(barrier, len(peers))
    loads[0].wait()
    tok_copy = remote(tok.at[tp], tok.at[tp], tok_send.at[0], tok_recv.at[0], partner)
    tok_copy.start()

    nsel_copies = []
    for n, (dz, dy) in enumerate(SERVED):
        c = remote(sel_v, nsel_v.at[n], nsel_send.at[n], nsel_recv.at[n], dev(-dz, -dy))
        c.start()
        nsel_copies.append(c)
    tabs = [
        pltpu.make_async_copy(sel_v, sel_s, tab_sem.at[0]),
        pltpu.make_async_copy(ent_v, ent_s, tab_sem.at[1]),
    ]
    for t in tabs:
        t.start()

    for load in small[1:]:
        load.wait()
    tok_copy.wait_recv()
    g0 = gain[:, 0:512]
    g1 = gain[:, 512:1024]

    def norm_rows(i, carry):
        at = pl.ds(i * 32, 32)
        a = tok[0, at, :].astype(F32)
        b = tok[1, at, :].astype(F32)
        total = jnp.sum(a * a + b * b, axis=1, keepdims=True)
        r = lax.rsqrt(total * (1.0 / 1024.0) + EPS)
        hid[at, 0:512] = (a * r * g0).astype(BF16)
        hid[at, 512:1024] = (b * r * g1).astype(BF16)
        return carry

    lax.fori_loop(0, 8, norm_rows, 0)
    loads[1].wait()
    loads[2].wait()
    kgain = jnp.concatenate([kg[...], kg[...]], axis=1)
    qgain = jnp.concatenate([qg[...], qg[...]], axis=1)
    both = jnp.dot(hid[...], wkv_v[...], preferred_element_type=F32)
    keys = head_norm(both[:, 0:128], kgain).astype(BF16)
    values = both[:, 128:256].astype(BF16)
    for k, rows_of in enumerate((keys, values)):
        blocks = rows_of.reshape(NB, BLK, 128)
        c0[:, :, 128 * k : 128 * (k + 1)] = blocks
        land[pl.ds(OWN, NB), :, 128 * k : 128 * (k + 1)] = blocks

    size = NB // CHUNKS

    def up(d, part):
        at = pl.ds(part * size, size)
        n = CHUNKS * d + part
        return remote(
            col[d].at[at], col[d + 1].at[at], up_send.at[n], up_recv.at[n], dev(1, 0)
        )

    def down(d, part):
        at = pl.ds(part * size, size)
        n = CHUNKS * d + part
        return remote(
            col[(8 - d) % 8].at[at], col[7 - d].at[at], dn_send.at[n], dn_recv.at[n], dev(-1, 0)
        )

    ups = [[up(d, bit) for bit in range(CHUNKS)] for d in range(4)]
    downs = [[down(d, bit) for bit in range(CHUNKS)] for d in range(3)]
    for bit in range(CHUNKS):
        ups[0][bit].start()
        downs[0][bit].start()
    plane_copies = []
    for dy in (1, 3, 2):
        c = remote(c0, plane[dy], pln_send.at[dy], pln_recv.at[dy], dev(0, dy))
        c.start()
        plane_copies.append(c)

    y_copies = {}

    def picked(table, source, d, dy, s):
        which = table[s, source * NB]
        return plane[dy][which] if d == 0 else col[d][which]

    def device_no(dz, dy):
        return ((z + dz + NZ) % NZ) * NY + (y + dy + NY) % NY

    def send(n, k, source, d, dy):
        for s in range(MOST):
            msg[k, s] = picked(nsel_s.at[n], source, d, dy, s)
        c = remote(
            msg.at[k], land.at[pl.ds(k * MOST, MOST)],
            y_send.at[k], y_recv.at[k], dev(*SERVED[n]),
        )
        c.start()
        y_copies[k] = c

    def serve(d):
        for n, dy in ((0, 1), (2, 3), (1, 2)):
            if not (d in (2, 6) and dy == 2):
                send(n, dy * NZ + d, device_no(-d, 0), d, 0)

    def keep(d, dy):
        for s in range(MOST):
            land[(dy * NZ + d) * MOST + s] = picked(sel_s, device_no(-d, -dy), d, dy, s)

    def turn(k):
        for bit in range(CHUNKS):
            ups[k - 1][bit].wait_recv()
            if k < 4:
                ups[k][bit].start()
                downs[k - 1][bit].wait_recv()
            if k < 3:
                downs[k][bit].start()

    for c in nsel_copies:
        c.wait_recv()
    ntab = [
        pltpu.make_async_copy(nsel_v.at[n], nsel_s.at[n], tab_sem.at[2 + n])
        for n in range(len(SERVED))
    ]
    for t in ntab:
        t.start()
    for t in tabs + ntab:
        t.wait()

    low_half = lax.broadcasted_iota(I32, (TOK, 128), 1) < HD

    def queries(one, two, pair, turned):
        flat = [
            jnp.dot(hid[...], wq_v[:, 128 * t : 128 * (t + 1)], preferred_element_type=F32)
            for t in (one, two)
        ]
        a, b = (head_norm(x, qgain) for x in flat)
        for (lo, hi), roll in ((pair, False), (turned, True)):
            if roll:
                a, b = pltpu.roll(a, HD, 1), pltpu.roll(b, HD, 1)
            first = jnp.where(low_half, a, 0.0).astype(BF16)
            second = jnp.where(low_half, 0.0, b).astype(BF16)
            for r in range(NB):
                qbd[r, pl.ds(lo * BLK, BLK), :] = first[r * BLK : (r + 1) * BLK]
                qbd[r, pl.ds(hi * BLK, BLK), :] = second[r * BLK : (r + 1) * BLK]

    turn(1)
    serve(1)
    keep(1, 0)
    keep(7, 0)
    loads[3].wait()
    queries(0, 2, PAIRS[0], PAIRS[2])
    turn(2)
    serve(2)
    serve(6)
    for c in plane_copies:
        c.wait_recv()
    for dy in (1, 2, 3):
        send(5, dy * NZ + 7, device_no(0, -dy), 0, dy)
    send(3, 2 * NZ + 2, device_no(0, -2), 0, 2)
    send(4, 2 * NZ + 6, device_no(0, -2), 0, 2)
    for dy in (1, 2, 3):
        keep(0, dy)
    keep(2, 0)
    keep(6, 0)
    queries(1, 3, PAIRS[1], PAIRS[3])
    turn(3)
    serve(3)
    serve(5)
    keep(3, 0)
    keep(5, 0)
    turn(4)
    serve(4)
    keep(4, 0)
    for load in loads[4:]:
        load.wait()
    for c in y_copies.values():
        c.wait_recv()

    def attend(r, carry):
        for e in range(TOPB):
            kvg[pl.ds(e * BLK, BLK), :] = land[ent_s[r, e]]
        raw = lax.dot_general(
            qbd[r], kvg[:, 0:128], (((1,), (1,)), ((), ())), preferred_element_type=F32
        )
        t = bias_t[...] + ((kv * NB + r) * BLK).astype(F32)
        a = bias_a[...]
        total = jnp.zeros((TOK, 128), F32)
        probs = []
        for i in range(4):
            u = upos[r, 0:1, 128 * i : 128 * (i + 1)]
            if i == 0:
                off = jnp.where(u > t, FAR, u - t)
            else:
                off = u - t
            w = jnp.exp2(raw[:, 128 * i : 128 * (i + 1)] * (LOG2E / 8.0) + a * off)
            total = total + w
            probs.append(w.astype(BF16))
        row_sum = jnp.sum(total, axis=1, keepdims=True)
        weighted = jnp.dot(
            jnp.concatenate(probs, axis=1), kvg[:, 128:256], preferred_element_type=F32
        )
        weighted = weighted / row_sum
        low = lax.broadcasted_iota(I32, (BLK, 128), 1) < HD
        for p, pair in enumerate(PAIRS):
            tile = jnp.where(
                low,
                weighted[pair[0] * BLK : (pair[0] + 1) * BLK],
                weighted[pair[1] * BLK : (pair[1] + 1) * BLK],
            )
            att[pl.ds(r * BLK, BLK), 128 * p : 128 * (p + 1)] = tile.astype(
                BF16
            )
        spot = lax.broadcasted_iota(I32, (TOK, 256), 1)
        query = lax.broadcasted_iota(I32, (TOK, 256), 0) % BLK
        lsum[...] = jnp.where(spot == r * BLK + query, row_sum, lsum[...])
        return carry

    out_copies = []
    for piece in range(PIECES):
        for r in range(piece * PER, (piece + 1) * PER):
            attend(r, 0)
        at = pl.ds(piece * PER * BLK, PER * BLK)
        rows_in = att[at, :]
        theirs = pl.multiple_of((1 - tp) * 512, 512)
        part[at, :] = jnp.dot(
            rows_in, wo_v[:, pl.ds(theirs, 512)], preferred_element_type=F32
        ).astype(BF16)
        c = remote(
            part.at[at, :], part_in.at[at, :], out_send.at[piece], out_recv.at[piece], partner
        )
        c.start()
        out_copies.append(c)
    logs[...] = jnp.log(jnp.sum(lsum[...].reshape(HEADS, BLK, 256), axis=1))
    mine = pl.multiple_of(tp * 512, 512)
    for piece in range(PIECES):
        at = pl.ds(piece * PER * BLK, PER * BLK)
        own = jnp.dot(att[at, :], wo_v[:, pl.ds(mine, 512)], preferred_element_type=F32)
        out_copies[piece].wait_recv()
        out[at, :] = (own + part_in[at, :].astype(F32)).astype(BF16)

    tok_copy.wait_send()
    for c in nsel_copies + plane_copies + out_copies + list(y_copies.values()):
        c.wait_send()
    for step in ups + downs:
        for c in step:
            c.wait_send()


def body(tokens, norm_gain, w_query, w_key, w_value, q_gain, k_gain, w_out, chosen):
    hbm = pl.BlockSpec(memory_space=pltpu.HBM)
    vmem = pl.BlockSpec(memory_space=pltpu.VMEM)
    dma = pltpu.SemaphoreType.DMA
    mixed, logs = pl.pallas_call(
        kernel,
        out_shape=(
            jax.ShapeDtypeStruct((TOK, 512), BF16),
            jax.ShapeDtypeStruct((HEADS, TOK), F32),
        ),
        in_specs=[hbm] * 9,
        out_specs=(vmem, vmem),
        scratch_shapes=[
            pltpu.VMEM((NB, TOPB), I32),
            pltpu.VMEM((1, 1024), F32),
            pltpu.VMEM((1, HD), F32),
            pltpu.VMEM((1, HD), F32),
            pltpu.VMEM((2, TOK, 512), BF16),
            pltpu.VMEM((TOK, 1024), BF16),
            pltpu.VMEM((1024, 512), BF16),
            pltpu.VMEM((1024, 256), BF16),
            pltpu.VMEM((512, 1024), BF16),
            *[pltpu.VMEM((NB, BLK, 256), BF16) for _ in range(11)],
            pltpu.VMEM((NZ * NY, MOST, BLK, 256), BF16),
            pltpu.VMEM((LANDED, BLK, 256), BF16),
            pltpu.VMEM((NB, 256), I32),
            pltpu.VMEM((len(SERVED), NB, 256), I32),
            pltpu.VMEM((NB, 128), I32),
            pltpu.SMEM((NB, 256), I32),
            pltpu.SMEM((len(SERVED), NB, 256), I32),
            pltpu.SMEM((NB, 128), I32),
            pltpu.VMEM((NB, 8, TOPB * BLK), F32),
            pltpu.VMEM((TOK, 128), F32),
            pltpu.VMEM((TOK, 128), F32),
            pltpu.VMEM((NB, TOK, 128), BF16),
            pltpu.VMEM((TOPB * BLK, 256), BF16),
            pltpu.VMEM((TOK, 512), BF16),
            pltpu.VMEM((TOK, 256), F32),
            pltpu.VMEM((TOK, 512), BF16),
            pltpu.VMEM((TOK, 512), BF16),
            dma((4,)),
            dma((12,)),
            dma((2 + len(SERVED),)),
            dma((1,)), dma((1,)),
            dma((len(SERVED),)), dma((len(SERVED),)),
            dma((4 * CHUNKS,)), dma((4 * CHUNKS,)),
            dma((3 * CHUNKS,)), dma((3 * CHUNKS,)),
            dma((NY,)), dma((NY,)),
            dma((NZ * NY,)), dma((NZ * NY,)),
            dma((PIECES,)), dma((PIECES,)),
        ],
        compiler_params=pltpu.CompilerParams(
            collective_id=0, has_side_effects=True, vmem_limit_bytes=60000 * 1024
        ),
        name="fused",
    )(
        tokens.reshape(TOK, 512),
        norm_gain.reshape(1, 1024),
        w_query,
        w_key,
        w_value,
        q_gain.reshape(1, HD),
        k_gain.reshape(1, HD),
        w_out,
        chosen.reshape(NB, TOPB),
    )
    return mixed.reshape(1, TOK, 512), logs.reshape(1, HEADS, TOK)


def solution(mesh):
    return jax.shard_map(
        body,
        mesh=mesh,
        in_specs=(
            P("dp", "kv", "tp"), P(), P(None, "tp"), P(None, "tp"), P(None, "tp"),
            P(), P(), P("tp", None), P("dp", "kv", None),
        ),
        out_specs=(P("dp", "kv", "tp"), P("dp", "tp", "kv")),
        check_vma=False,
    )
```

```python
import functools
import math

import jax
import jax.numpy as jnp
from jax import lax
from jax.experimental import pallas as pl
from jax.experimental.pallas import tpu as pltpu
from jax.sharding import PartitionSpec as P

MESH = pl.DeviceIdType.MESH
F32 = jnp.float32
BF16 = jnp.bfloat16
I32 = jnp.int32

NZ, NY = 8, 4
NB = 8
BLK = 32
TOPB = 16
MOST = 4
HD = 64
HEADS = 8
TOK = NB * BLK
EPS = 1e-6
SEQ = 8192
OWN = NZ * NY * MOST
LANDED = OWN + NB
FAR = -1e30
PAIRS = ((0, 5), (2, 7), (1, 4), (3, 6))
NEAR = ((0, 1), (0, 2), (0, 3), (1, 0), (-1, 0), (2, 0), (-2, 0))
SERVED = ((0, 1), (0, 2), (0, 3), (2, 0), (-2, 0), (-1, 0))
CHUNKS = 4
STEP = TOK // CHUNKS
PIECES = 2
PER = NB // PIECES
LOG2E = math.log2(math.e)


def half_sums(x):
    row = lax.broadcasted_iota(I32, (128, 128), 0) // HD
    col = lax.broadcasted_iota(I32, (128, 128), 1) // HD
    ones = jnp.where(row == col, 1.0, 0.0).astype(BF16)
    high = x.astype(BF16)
    low = (x - high.astype(F32)).astype(BF16)
    return jnp.dot(high, ones, preferred_element_type=F32) + jnp.dot(
        low, ones, preferred_element_type=F32
    )


def head_norm(x, gain):
    return x * lax.rsqrt(half_sums(x * x) * (1.0 / HD) + EPS) * gain


def kernel(
    tokens, gain_h, wq, wk, wv, qg_h, kg_h, wo, chosen_h,
    out, logs,
    chosen, gain, qg, kg, tok, hid, wq_v, wkv_v, wo_v,
    c0, c1, c2, c3, c4, c5, c6, c7, p1, p2, p3,
    msg, land, sel_v, nsel_v, ent_v, sel_s, nsel_s, ent_s,
    upos, bias_t, bias_a, qbd, kvg, att, lsum, part, part_in,
    small_sem, load_sem, tab_sem, tok_send, tok_recv, nsel_send, nsel_recv,
    up_send, up_recv, dn_send, dn_recv, pln_send, pln_recv, y_send, y_recv, out_send, out_recv,
):
    dp = lax.axis_index("dp")
    kv = lax.axis_index("kv")
    tp = lax.axis_index("tp")
    z = kv // NY
    y = kv % NY
    col = (c0, c1, c2, c3, c4, c5, c6, c7)
    plane = (c0, p1, p2, p3)

    def dev(dz, dy):
        return (dp, ((z + dz) % NZ) * NY + (y + dy) % NY, tp)

    partner = (dp, kv, 1 - tp)

    def remote(src, dst, send, recv, where):
        return pltpu.make_async_remote_copy(
            src_ref=src, dst_ref=dst, send_sem=send, recv_sem=recv,
            device_id=where, device_id_type=MESH,
        )

    barrier = pltpu.get_barrier_semaphore()
    peers = [partner] + [dev(*at) for at in NEAR]
    for peer in peers:
        pl.semaphore_signal(barrier, inc=1, device_id=peer, device_id_type=MESH)

    small = [
        pltpu.make_async_copy(src, dst, small_sem.at[n])
        for n, (src, dst) in enumerate(
            ((chosen_h, chosen), (gain_h, gain), (qg_h, qg), (kg_h, kg))
        )
    ]
    for load in small:
        load.start()
    loads = [
        pltpu.make_async_copy(tokens, tok.at[tp], load_sem.at[0]),
        pltpu.make_async_copy(wk, wkv_v.at[:, pl.ds(0, 128)], load_sem.at[1]),
        pltpu.make_async_copy(wv, wkv_v.at[:, pl.ds(128, 128)], load_sem.at[2]),
        pltpu.make_async_copy(wq, wq_v, load_sem.at[3]),
    ]
    for p, pair in enumerate(PAIRS):
        for side in range(2):
            loads.append(
                pltpu.make_async_copy(
                    wo.at[pl.ds(pair[side] * HD, HD), :],
                    wo_v.at[pl.ds(p * 128 + side * HD, HD), :],
                    load_sem.at[4 + 2 * p + side],
                )
            )
    for load in loads:
        load.start()

    small[0].wait()
    ch = chosen[...]
    lane = lax.broadcasted_iota(I32, (NB, 256), 1)
    own_block = kv * NB + lax.broadcasted_iota(I32, (NB, 1), 0)
    member = jnp.zeros((NB, 256), I32)
    for e in range(TOPB):
        member = jnp.where(ch[:, e : e + 1] == lane, 1, member)
    present = jnp.broadcast_to(jnp.max(member, axis=0, keepdims=True), (NB, 256))
    inner = lane % NB
    rank = jnp.zeros((NB, 256), I32)
    for k in range(1, NB):
        rank = rank + jnp.where(inner >= k, pltpu.roll(present, k, 1), 0)
    sub = lax.broadcasted_iota(I32, (NB, 256), 0)
    sel = jnp.zeros((NB, 256), I32)
    for s in range(MOST):
        val = jnp.where((present == 1) & (rank == s), inner, 0)
        for k in (1, 2, 4):
            val = val + pltpu.roll(val, 256 - k, 1)
        sel = jnp.where(sub == s, val, sel)
    sel_v[...] = sel
    chip = lane // NB
    from_y = (y - chip % NY + NY) % NY
    from_z = (z - chip // NY + NZ) % NZ
    spot_of = jnp.where(
        chip == kv,
        OWN + inner,
        (from_y * NZ + from_z) * MOST + rank,
    )
    front = jnp.where(
        lax.broadcasted_iota(I32, (NB, TOPB), 1) == 0,
        own_block,
        jnp.where(ch == own_block, ch[:, 0:1], ch),
    )
    filled = jnp.where(front < 0, own_block, front)
    lane_e = lax.broadcasted_iota(I32, (NB, 128), 1)
    entry = jnp.zeros((NB, 128), I32)
    lane_u = lax.broadcasted_iota(I32, (NB, TOPB * BLK), 1)
    pos = jnp.full((NB, TOPB * BLK), FAR, F32)
    for e in range(TOPB):
        at = jnp.sum(jnp.where(filled[:, e : e + 1] == lane, spot_of, 0), axis=1, keepdims=True)
        entry = jnp.where(lane_e == e, at, entry)
        first = front[:, e : e + 1]
        pos = jnp.where(
            (lane_u // BLK == e) & (first >= 0),
            (first * BLK + lane_u % BLK).astype(F32),
            pos,
        )
    ent_v[...] = entry
    for r in range(NB):
        upos[r] = jnp.broadcast_to(pos[r : r + 1], (8, TOPB * BLK))

    rows = lax.broadcasted_iota(I32, (TOK, 128), 0)
    head_no = (tp * HEADS + rows // BLK + 1).astype(F32)
    bias_t[...] = (rows % BLK).astype(F32)
    bias_a[...] = jnp.exp2(head_no * (-8.0 / 16.0)) * (4.0 / SEQ * LOG2E)

    pl.semaphore_wait(barrier, len(peers))
    loads[0].wait()
    tok_copies = []
    for i in range(CHUNKS):
        at = pl.ds(i * STEP, STEP)
        c = remote(tok.at[tp, at], tok.at[tp, at], tok_send.at[i], tok_recv.at[i], partner)
        c.start()
        tok_copies.append(c)

    nsel_copies = []
    for n, (dz, dy) in enumerate(SERVED):
        c = remote(sel_v, nsel_v.at[n], nsel_send.at[n], nsel_recv.at[n], dev(-dz, -dy))
        c.start()
        nsel_copies.append(c)
    tabs = [
        pltpu.make_async_copy(sel_v, sel_s, tab_sem.at[0]),
        pltpu.make_async_copy(ent_v, ent_s, tab_sem.at[1]),
    ]
    for t in tabs:
        t.start()

    for load in small[1:]:
        load.wait()
    size = NB // CHUNKS

    def up(d, part):
        at = pl.ds(part * size, size)
        n = CHUNKS * d + part
        return remote(
            col[d].at[at], col[d + 1].at[at], up_send.at[n], up_recv.at[n], dev(1, 0)
        )

    def down(d, part):
        at = pl.ds(part * size, size)
        n = CHUNKS * d + part
        return remote(
            col[(8 - d) % 8].at[at], col[7 - d].at[at], dn_send.at[n], dn_recv.at[n], dev(-1, 0)
        )

    ups = [[up(d, bit) for bit in range(CHUNKS)] for d in range(4)]
    downs = [[down(d, bit) for bit in range(CHUNKS)] for d in range(3)]
    g0 = gain[:, 0:512]
    g1 = gain[:, 512:1024]
    kgain = jnp.concatenate([kg[...], kg[...]], axis=1)
    qgain = jnp.concatenate([qg[...], qg[...]], axis=1)
    loads[1].wait()
    loads[2].wait()
    plane_copies = []
    for i in range(CHUNKS):
        tok_copies[i].wait_recv()
        for half in range(2):
            at = pl.ds(i * STEP + half * (STEP // 2), STEP // 2)
            a = tok[0, at, :].astype(F32)
            b = tok[1, at, :].astype(F32)
            total = jnp.sum(a * a + b * b, axis=1, keepdims=True)
            r = lax.rsqrt(total * (1.0 / 1024.0) + EPS)
            hid[at, 0:512] = (a * r * g0).astype(BF16)
            hid[at, 512:1024] = (b * r * g1).astype(BF16)
        both = jnp.dot(hid[pl.ds(i * STEP, STEP), :], wkv_v[...], preferred_element_type=F32)
        keys = head_norm(both[:, 0:128], kgain).astype(BF16)
        values = both[:, 128:256].astype(BF16)
        for k, rows_of in enumerate((keys, values)):
            blocks = rows_of.reshape(size, BLK, 128)
            c0[pl.ds(i * size, size), :, 128 * k : 128 * (k + 1)] = blocks
            land[pl.ds(OWN + i * size, size), :, 128 * k : 128 * (k + 1)] = blocks
        ups[0][i].start()
        downs[0][i].start()
        for dy in (1, 3, 2):
            at = pl.ds(i * size, size)
            n = dy * CHUNKS + i
            c = remote(c0.at[at], plane[dy].at[at], pln_send.at[n], pln_recv.at[n], dev(0, dy))
            c.start()
            plane_copies.append(c)

    y_copies = {}

    def picked(table, source, d, dy, s):
        which = table[s, source * NB]
        return plane[dy][which] if d == 0 else col[d][which]

    def device_no(dz, dy):
        return ((z + dz + NZ) % NZ) * NY + (y + dy + NY) % NY

    def send(n, k, source, d, dy):
        for s in range(MOST):
            msg[k, s] = picked(nsel_s.at[n], source, d, dy, s)
        c = remote(
            msg.at[k], land.at[pl.ds(k * MOST, MOST)],
            y_send.at[k], y_recv.at[k], dev(*SERVED[n]),
        )
        c.start()
        y_copies[k] = c

    def serve(d):
        for n, dy in ((0, 1), (2, 3), (1, 2)):
            if not (d in (2, 6) and dy == 2):
                send(n, dy * NZ + d, device_no(-d, 0), d, 0)

    def keep(d, dy):
        for s in range(MOST):
            land[(dy * NZ + d) * MOST + s] = picked(sel_s, device_no(-d, -dy), d, dy, s)

    def turn(k):
        for bit in range(CHUNKS):
            ups[k - 1][bit].wait_recv()
            if k < 4:
                ups[k][bit].start()
                downs[k - 1][bit].wait_recv()
            if k < 3:
                downs[k][bit].start()

    for c in nsel_copies:
        c.wait_recv()
    ntab = [
        pltpu.make_async_copy(nsel_v.at[n], nsel_s.at[n], tab_sem.at[2 + n])
        for n in range(len(SERVED))
    ]
    for t in ntab:
        t.start()
    for t in tabs + ntab:
        t.wait()

    low_half = lax.broadcasted_iota(I32, (TOK, 128), 1) < HD

    def queries(one, two, pair, turned):
        flat = [
            jnp.dot(hid[...], wq_v[:, 128 * t : 128 * (t + 1)], preferred_element_type=F32)
            for t in (one, two)
        ]
        a, b = (head_norm(x, qgain) for x in flat)
        for (lo, hi), roll in ((pair, False), (turned, True)):
            if roll:
                a, b = pltpu.roll(a, HD, 1), pltpu.roll(b, HD, 1)
            first = jnp.where(low_half, a, 0.0).astype(BF16)
            second = jnp.where(low_half, 0.0, b).astype(BF16)
            for r in range(NB):
                qbd[r, pl.ds(lo * BLK, BLK), :] = first[r * BLK : (r + 1) * BLK]
                qbd[r, pl.ds(hi * BLK, BLK), :] = second[r * BLK : (r + 1) * BLK]

    turn(1)
    serve(1)
    keep(1, 0)
    keep(7, 0)
    loads[3].wait()
    queries(0, 2, PAIRS[0], PAIRS[2])
    turn(2)
    serve(2)
    serve(6)
    for c in plane_copies:
        c.wait_recv()
    for dy in (1, 2, 3):
        send(5, dy * NZ + 7, device_no(0, -dy), 0, dy)
    send(3, 2 * NZ + 2, device_no(0, -2), 0, 2)
    send(4, 2 * NZ + 6, device_no(0, -2), 0, 2)
    for dy in (1, 2, 3):
        keep(0, dy)
    keep(2, 0)
    keep(6, 0)
    queries(1, 3, PAIRS[1], PAIRS[3])
    turn(3)
    serve(3)
    serve(5)
    keep(3, 0)
    keep(5, 0)
    turn(4)
    serve(4)
    keep(4, 0)
    for load in loads[4:]:
        load.wait()
    for c in y_copies.values():
        c.wait_recv()

    def attend(r, carry):
        for e in range(TOPB):
            kvg[pl.ds(e * BLK, BLK), :] = land[ent_s[r, e]]
        raw = lax.dot_general(
            qbd[r], kvg[:, 0:128], (((1,), (1,)), ((), ())), preferred_element_type=F32
        )
        t = bias_t[...] + ((kv * NB + r) * BLK).astype(F32)
        a = bias_a[...]
        total = jnp.zeros((TOK, 128), F32)
        probs = []
        for i in range(4):
            u = upos[r, 0:1, 128 * i : 128 * (i + 1)]
            if i == 0:
                off = jnp.where(u > t, FAR, u - t)
            else:
                off = u - t
            w = jnp.exp2(raw[:, 128 * i : 128 * (i + 1)] * (LOG2E / 8.0) + a * off)
            total = total + w
            probs.append(w.astype(BF16))
        row_sum = jnp.sum(total, axis=1, keepdims=True)
        weighted = jnp.dot(
            jnp.concatenate(probs, axis=1), kvg[:, 128:256], preferred_element_type=F32
        )
        weighted = weighted / row_sum
        low = lax.broadcasted_iota(I32, (BLK, 128), 1) < HD
        for p, pair in enumerate(PAIRS):
            tile = jnp.where(
                low,
                weighted[pair[0] * BLK : (pair[0] + 1) * BLK],
                weighted[pair[1] * BLK : (pair[1] + 1) * BLK],
            )
            att[pl.ds(pl.multiple_of(r * BLK, BLK), BLK), 128 * p : 128 * (p + 1)] = tile.astype(
                BF16
            )
        lsum[r] = jnp.broadcast_to(row_sum, (TOK, 128))
        return carry

    def out_copy(piece):
        return remote(
            part.at[piece], part_in.at[piece], out_send.at[piece], out_recv.at[piece], partner
        )

    def do_piece(piece, carry):
        for r in range(PER):
            attend(piece * PER + r, 0)
        at = pl.ds(pl.multiple_of(piece * PER * BLK, PER * BLK), PER * BLK)
        theirs = pl.multiple_of((1 - tp) * 512, 512)
        part[piece] = jnp.dot(
            att[at, :], wo_v[:, pl.ds(theirs, 512)], preferred_element_type=F32
        ).astype(BF16)
        out_copy(piece).start()
        return carry

    lax.fori_loop(0, PIECES, do_piece, 0)
    out_copies = [out_copy(piece) for piece in range(PIECES)]
    lane_q = lax.broadcasted_iota(I32, (TOK, 128), 1)
    query = lax.broadcasted_iota(I32, (TOK, 128), 0) % BLK
    for side in range(2):
        sums = jnp.zeros((TOK, 128), F32)
        for r in range(4):
            sums = jnp.where(lane_q == r * BLK + query, lsum[4 * side + r], sums)
        logs[:, 128 * side : 128 * (side + 1)] = jnp.log(
            jnp.sum(sums.reshape(HEADS, BLK, 128), axis=1)
        )
    mine = pl.multiple_of(tp * 512, 512)
    for piece in range(PIECES):
        at = pl.ds(piece * PER * BLK, PER * BLK)
        own = jnp.dot(att[at, :], wo_v[:, pl.ds(mine, 512)], preferred_element_type=F32)
        out_copies[piece].wait_recv()
        out[at, :] = (own + part_in[piece].astype(F32)).astype(BF16)

    for c in tok_copies + nsel_copies + plane_copies + out_copies + list(y_copies.values()):
        c.wait_send()
    for step in ups + downs:
        for c in step:
            c.wait_send()


def body(tokens, norm_gain, w_query, w_key, w_value, q_gain, k_gain, w_out, chosen):
    hbm = pl.BlockSpec(memory_space=pltpu.HBM)
    vmem = pl.BlockSpec(memory_space=pltpu.VMEM)
    dma = pltpu.SemaphoreType.DMA
    mixed, logs = pl.pallas_call(
        kernel,
        out_shape=(
            jax.ShapeDtypeStruct((TOK, 512), BF16),
            jax.ShapeDtypeStruct((HEADS, TOK), F32),
        ),
        in_specs=[hbm] * 9,
        out_specs=(vmem, vmem),
        scratch_shapes=[
            pltpu.VMEM((NB, TOPB), I32),
            pltpu.VMEM((1, 1024), F32),
            pltpu.VMEM((1, HD), F32),
            pltpu.VMEM((1, HD), F32),
            pltpu.VMEM((2, TOK, 512), BF16),
            pltpu.VMEM((TOK, 1024), BF16),
            pltpu.VMEM((1024, 512), BF16),
            pltpu.VMEM((1024, 256), BF16),
            pltpu.VMEM((512, 1024), BF16),
            *[pltpu.VMEM((NB, BLK, 256), BF16) for _ in range(11)],
            pltpu.VMEM((NZ * NY, MOST, BLK, 256), BF16),
            pltpu.VMEM((LANDED, BLK, 256), BF16),
            pltpu.VMEM((NB, 256), I32),
            pltpu.VMEM((len(SERVED), NB, 256), I32),
            pltpu.VMEM((NB, 128), I32),
            pltpu.SMEM((NB, 256), I32),
            pltpu.SMEM((len(SERVED), NB, 256), I32),
            pltpu.SMEM((NB, 128), I32),
            pltpu.VMEM((NB, 8, TOPB * BLK), F32),
            pltpu.VMEM((TOK, 128), F32),
            pltpu.VMEM((TOK, 128), F32),
            pltpu.VMEM((NB, TOK, 128), BF16),
            pltpu.VMEM((TOPB * BLK, 256), BF16),
            pltpu.VMEM((TOK, 512), BF16),
            pltpu.VMEM((NB, TOK, 128), F32),
            pltpu.VMEM((PIECES, PER * BLK, 512), BF16),
            pltpu.VMEM((PIECES, PER * BLK, 512), BF16),
            dma((4,)),
            dma((12,)),
            dma((2 + len(SERVED),)),
            dma((CHUNKS,)), dma((CHUNKS,)),
            dma((len(SERVED),)), dma((len(SERVED),)),
            dma((4 * CHUNKS,)), dma((4 * CHUNKS,)),
            dma((3 * CHUNKS,)), dma((3 * CHUNKS,)),
            dma((NY * CHUNKS,)), dma((NY * CHUNKS,)),
            dma((NZ * NY,)), dma((NZ * NY,)),
            dma((PIECES,)), dma((PIECES,)),
        ],
        compiler_params=pltpu.CompilerParams(
            collective_id=0, has_side_effects=True, vmem_limit_bytes=54700 * 1024
        ),
        name="fused",
    )(
        tokens.reshape(TOK, 512),
        norm_gain.reshape(1, 1024),
        w_query,
        w_key,
        w_value,
        q_gain.reshape(1, HD),
        k_gain.reshape(1, HD),
        w_out,
        chosen.reshape(NB, TOPB),
    )
    return mixed.reshape(1, TOK, 512), logs.reshape(1, HEADS, TOK)


def solution(mesh):
    return jax.shard_map(
        body,
        mesh=mesh,
        in_specs=(
            P("dp", "kv", "tp"), P(), P(None, "tp"), P(None, "tp"), P(None, "tp"),
            P(), P(), P("tp", None), P("dp", "kv", None),
        ),
        out_specs=(P("dp", "kv", "tp"), P("dp", "tp", "kv")),
        check_vma=False,
    )
```

```python
import functools
import math

import jax
import jax.numpy as jnp
from jax import lax
from jax.experimental import pallas as pl
from jax.experimental.pallas import tpu as pltpu
from jax.sharding import PartitionSpec as P

MESH = pl.DeviceIdType.MESH
F32 = jnp.float32
BF16 = jnp.bfloat16
I32 = jnp.int32

NZ, NY = 8, 4
NB = 8
BLK = 32
TOPB = 16
MOST = 4
HD = 64
HEADS = 8
TOK = NB * BLK
EPS = 1e-6
SEQ = 8192
OWN = NZ * NY * MOST
LANDED = OWN + NB
FAR = -1e30
PAIRS = ((0, 5), (2, 7), (1, 4), (3, 6))
NEAR = ((0, 1), (0, 2), (0, 3), (1, 0), (-1, 0), (2, 0), (-2, 0))
SERVED = ((0, 1), (0, 2), (0, 3), (2, 0), (-2, 0), (-1, 0))
CHUNKS = 4
STEP = TOK // CHUNKS
PIECES = 2
PER = NB // PIECES
LOG2E = math.log2(math.e)


def half_sums(x):
    row = lax.broadcasted_iota(I32, (128, 128), 0) // HD
    col = lax.broadcasted_iota(I32, (128, 128), 1) // HD
    ones = jnp.where(row == col, 1.0, 0.0).astype(BF16)
    high = x.astype(BF16)
    low = (x - high.astype(F32)).astype(BF16)
    return jnp.dot(high, ones, preferred_element_type=F32) + jnp.dot(
        low, ones, preferred_element_type=F32
    )


def head_norm(x, gain):
    return x * lax.rsqrt(half_sums(x * x) * (1.0 / HD) + EPS) * gain


def kernel(
    tokens, gain_h, wq, wk, wv, qg_h, kg_h, wo, chosen_h,
    out, logs,
    chosen, gain, qg, kg, tok, hid, wq_v, wkv_v, wo_v,
    c0, c1, c2, c3, c4, c5, c6, c7, p1, p2, p3,
    msg, land, sel_v, nsel_v, ent_v, sel_s, nsel_s, ent_s,
    upos, slope, qbd, kvg, att, lsum, part, part_in,
    small_sem, mine_sem, load_sem, tab_sem, tok_send, tok_recv, nsel_send, nsel_recv,
    up_send, up_recv, dn_send, dn_recv, pln_send, pln_recv, y_send, y_recv, out_send, out_recv,
):
    dp = lax.axis_index("dp")
    kv = lax.axis_index("kv")
    tp = lax.axis_index("tp")
    z = kv // NY
    y = kv % NY
    col = (c0, c1, c2, c3, c4, c5, c6, c7)
    plane = (c0, p1, p2, p3)

    def dev(dz, dy):
        return (dp, ((z + dz) % NZ) * NY + (y + dy) % NY, tp)

    partner = (dp, kv, 1 - tp)

    def remote(src, dst, send, recv, where):
        return pltpu.make_async_remote_copy(
            src_ref=src, dst_ref=dst, send_sem=send, recv_sem=recv,
            device_id=where, device_id_type=MESH,
        )

    barrier = pltpu.get_barrier_semaphore()
    peers = [partner] + [dev(*at) for at in NEAR]
    for peer in peers:
        pl.semaphore_signal(barrier, inc=1, device_id=peer, device_id_type=MESH)

    small = [
        pltpu.make_async_copy(src, dst, small_sem.at[n])
        for n, (src, dst) in enumerate(
            ((chosen_h, chosen), (gain_h, gain), (qg_h, qg), (kg_h, kg))
        )
    ]
    for load in small:
        load.start()
    tok_loads = [
        pltpu.make_async_copy(
            tokens.at[pl.ds(i * STEP, STEP)], tok.at[tp, pl.ds(i * STEP, STEP)], mine_sem.at[i]
        )
        for i in range(CHUNKS)
    ]
    loads = [
        pltpu.make_async_copy(wk, wkv_v.at[:, pl.ds(0, 128)], load_sem.at[0]),
        pltpu.make_async_copy(wv, wkv_v.at[:, pl.ds(128, 128)], load_sem.at[1]),
        pltpu.make_async_copy(wq, wq_v, load_sem.at[2]),
    ]
    for p, pair in enumerate(PAIRS):
        for side in range(2):
            loads.append(
                pltpu.make_async_copy(
                    wo.at[pl.ds(pair[side] * HD, HD), :],
                    wo_v.at[pl.ds(p * 128 + side * HD, HD), :],
                    load_sem.at[3 + 2 * p + side],
                )
            )
    for load in tok_loads + loads:
        load.start()

    small[0].wait()
    ch = chosen[...]
    lane = lax.broadcasted_iota(I32, (NB, 256), 1)
    own_block = kv * NB + lax.broadcasted_iota(I32, (NB, 1), 0)
    member = jnp.zeros((NB, 256), I32)
    for e in range(TOPB):
        member = jnp.where(ch[:, e : e + 1] == lane, 1, member)
    present = jnp.broadcast_to(jnp.max(member, axis=0, keepdims=True), (NB, 256))
    inner = lane % NB
    rank = jnp.zeros((NB, 256), I32)
    for k in range(1, NB):
        rank = rank + jnp.where(inner >= k, pltpu.roll(present, k, 1), 0)
    sub = lax.broadcasted_iota(I32, (NB, 256), 0)
    sel = jnp.zeros((NB, 256), I32)
    for s in range(MOST):
        val = jnp.where((present == 1) & (rank == s), inner, 0)
        for k in (1, 2, 4):
            val = val + pltpu.roll(val, 256 - k, 1)
        sel = jnp.where(sub == s, val, sel)
    sel_v[...] = sel
    chip = lane // NB
    from_y = (y - chip % NY + NY) % NY
    from_z = (z - chip // NY + NZ) % NZ
    spot_of = jnp.where(
        chip == kv,
        OWN + inner,
        (from_y * NZ + from_z) * MOST + rank,
    )
    front = jnp.where(
        lax.broadcasted_iota(I32, (NB, TOPB), 1) == 0,
        own_block,
        jnp.where(ch == own_block, ch[:, 0:1], ch),
    )
    filled = jnp.where(front < 0, own_block, front)
    lane_e = lax.broadcasted_iota(I32, (NB, 128), 1)
    entry = jnp.zeros((NB, 128), I32)
    lane_u = lax.broadcasted_iota(I32, (NB, TOPB * BLK), 1)
    pos = jnp.full((NB, TOPB * BLK), FAR, F32)
    for e in range(TOPB):
        at = jnp.sum(jnp.where(filled[:, e : e + 1] == lane, spot_of, 0), axis=1, keepdims=True)
        entry = jnp.where(lane_e == e, at, entry)
        first = front[:, e : e + 1]
        pos = jnp.where(
            (lane_u // BLK == e) & (first >= 0),
            (first * BLK + lane_u % BLK).astype(F32),
            pos,
        )
    ent_v[...] = entry
    for r in range(NB):
        upos[r] = jnp.broadcast_to(pos[r : r + 1], (8, TOPB * BLK))

    head_no = (tp * HEADS + lax.broadcasted_iota(I32, (HEADS, 128), 0) + 1).astype(F32)
    slope[...] = jnp.exp2(head_no * (-8.0 / 16.0)) * (4.0 / SEQ * LOG2E)
    pl.semaphore_wait(barrier, len(peers))
    tok_copies = []
    for i in range(CHUNKS):
        at = pl.ds(i * STEP, STEP)
        tok_loads[i].wait()
        c = remote(tok.at[tp, at], tok.at[tp, at], tok_send.at[i], tok_recv.at[i], partner)
        c.start()
        tok_copies.append(c)

    nsel_copies = []
    for n, (dz, dy) in enumerate(SERVED):
        c = remote(sel_v, nsel_v.at[n], nsel_send.at[n], nsel_recv.at[n], dev(-dz, -dy))
        c.start()
        nsel_copies.append(c)
    tabs = [
        pltpu.make_async_copy(sel_v, sel_s, tab_sem.at[0]),
        pltpu.make_async_copy(ent_v, ent_s, tab_sem.at[1]),
    ]
    for t in tabs:
        t.start()

    for load in small[1:]:
        load.wait()
    size = NB // CHUNKS

    def up(d, part):
        at = pl.ds(part * size, size)
        n = CHUNKS * d + part
        return remote(
            col[d].at[at], col[d + 1].at[at], up_send.at[n], up_recv.at[n], dev(1, 0)
        )

    def down(d, part):
        at = pl.ds(part * size, size)
        n = CHUNKS * d + part
        return remote(
            col[(8 - d) % 8].at[at], col[7 - d].at[at], dn_send.at[n], dn_recv.at[n], dev(-1, 0)
        )

    ups = [[up(d, bit) for bit in range(CHUNKS)] for d in range(4)]
    downs = [[down(d, bit) for bit in range(CHUNKS)] for d in range(3)]
    g0 = gain[:, 0:512]
    g1 = gain[:, 512:1024]
    kgain = jnp.concatenate([kg[...], kg[...]], axis=1)
    qgain = jnp.concatenate([qg[...], qg[...]], axis=1)
    loads[0].wait()
    loads[1].wait()
    plane_copies = []
    for i in range(CHUNKS):
        tok_copies[i].wait_recv()
        for half in range(2):
            at = pl.ds(i * STEP + half * (STEP // 2), STEP // 2)
            a = tok[0, at, :].astype(F32)
            b = tok[1, at, :].astype(F32)
            total = jnp.sum(a * a + b * b, axis=1, keepdims=True)
            r = lax.rsqrt(total * (1.0 / 1024.0) + EPS)
            hid[at, 0:512] = (a * r * g0).astype(BF16)
            hid[at, 512:1024] = (b * r * g1).astype(BF16)
        both = jnp.dot(hid[pl.ds(i * STEP, STEP), :], wkv_v[...], preferred_element_type=F32)
        keys = head_norm(both[:, 0:128], kgain).astype(BF16)
        values = both[:, 128:256].astype(BF16)
        for k, rows_of in enumerate((keys, values)):
            blocks = rows_of.reshape(size, BLK, 128)
            c0[pl.ds(i * size, size), :, 128 * k : 128 * (k + 1)] = blocks
            land[pl.ds(OWN + i * size, size), :, 128 * k : 128 * (k + 1)] = blocks
        ups[0][i].start()
        downs[0][i].start()
        for dy in (1, 3, 2):
            at = pl.ds(i * size, size)
            n = dy * CHUNKS + i
            c = remote(c0.at[at], plane[dy].at[at], pln_send.at[n], pln_recv.at[n], dev(0, dy))
            c.start()
            plane_copies.append(c)

    y_copies = {}

    def picked(table, source, d, dy, s):
        which = table[s, source * NB]
        return plane[dy][which] if d == 0 else col[d][which]

    def device_no(dz, dy):
        return ((z + dz + NZ) % NZ) * NY + (y + dy + NY) % NY

    def send(n, k, source, d, dy):
        for s in range(MOST):
            msg[k, s] = picked(nsel_s.at[n], source, d, dy, s)
        c = remote(
            msg.at[k], land.at[pl.ds(k * MOST, MOST)],
            y_send.at[k], y_recv.at[k], dev(*SERVED[n]),
        )
        c.start()
        y_copies[k] = c

    def serve(d):
        for n, dy in ((0, 1), (2, 3), (1, 2)):
            if not (d in (2, 6) and dy == 2):
                send(n, dy * NZ + d, device_no(-d, 0), d, 0)

    def keep(d, dy):
        for s in range(MOST):
            land[(dy * NZ + d) * MOST + s] = picked(sel_s, device_no(-d, -dy), d, dy, s)

    def turn(k):
        for bit in range(CHUNKS):
            ups[k - 1][bit].wait_recv()
            if k < 4:
                ups[k][bit].start()
                downs[k - 1][bit].wait_recv()
            if k < 3:
                downs[k][bit].start()

    for c in nsel_copies:
        c.wait_recv()
    ntab = [
        pltpu.make_async_copy(nsel_v.at[n], nsel_s.at[n], tab_sem.at[2 + n])
        for n in range(len(SERVED))
    ]
    for t in ntab:
        t.start()
    for t in tabs + ntab:
        t.wait()

    low_half = lax.broadcasted_iota(I32, (TOK, 128), 1) < HD

    def queries(one, two, pair, turned):
        flat = [
            jnp.dot(hid[...], wq_v[:, 128 * t : 128 * (t + 1)], preferred_element_type=F32)
            for t in (one, two)
        ]
        a, b = (head_norm(x, qgain) for x in flat)
        for (lo, hi), roll in ((pair, False), (turned, True)):
            if roll:
                a, b = pltpu.roll(a, HD, 1), pltpu.roll(b, HD, 1)
            first = jnp.where(low_half, a, 0.0).astype(BF16)
            second = jnp.where(low_half, 0.0, b).astype(BF16)
            for r in range(NB):
                qbd[r, pl.ds(lo * BLK, BLK), :] = first[r * BLK : (r + 1) * BLK]
                qbd[r, pl.ds(hi * BLK, BLK), :] = second[r * BLK : (r + 1) * BLK]

    turn(1)
    serve(1)
    keep(1, 0)
    keep(7, 0)
    loads[2].wait()
    queries(0, 2, PAIRS[0], PAIRS[2])
    turn(2)
    serve(2)
    serve(6)
    for c in plane_copies:
        c.wait_recv()
    for dy in (1, 2, 3):
        send(5, dy * NZ + 7, device_no(0, -dy), 0, dy)
    send(3, 2 * NZ + 2, device_no(0, -2), 0, 2)
    send(4, 2 * NZ + 6, device_no(0, -2), 0, 2)
    for dy in (1, 2, 3):
        keep(0, dy)
    keep(2, 0)
    keep(6, 0)
    queries(1, 3, PAIRS[1], PAIRS[3])
    turn(3)
    serve(3)
    serve(5)
    keep(3, 0)
    keep(5, 0)
    turn(4)
    serve(4)
    keep(4, 0)
    for load in loads[3:]:
        load.wait()
    for c in y_copies.values():
        c.wait_recv()

    def attend(r, carry):
        for e in range(TOPB):
            kvg[pl.ds(e * BLK, BLK), :] = land[ent_s[r, e]]
        raw = lax.dot_general(
            qbd[r], kvg[:, 0:128], (((1,), (1,)), ((), ())), preferred_element_type=F32
        )
        total = jnp.zeros((TOK, 128), F32)
        probs = []
        first_key = (kv * NB + r) * BLK
        later = lax.broadcasted_iota(I32, (BLK, 128), 1) > lax.broadcasted_iota(
            I32, (BLK, 128), 0
        )
        own_lane = lax.broadcasted_iota(I32, (BLK, 128), 1) < BLK
        for i in range(4):
            off = upos[r, :, 128 * i : 128 * (i + 1)] - first_key.astype(F32)
            factor = jnp.exp2(slope[...] * off)
            w = jnp.exp2(raw[:, 128 * i : 128 * (i + 1)] * (LOG2E / 8.0)).reshape(
                HEADS, BLK, 128
            ) * factor.reshape(HEADS, 1, 128)
            if i == 0:
                w = jnp.where((later & own_lane)[None], 0.0, w)
            w = w.reshape(TOK, 128)
            total = total + w
            probs.append(w.astype(BF16))
        row_sum = jnp.sum(total, axis=1, keepdims=True)
        weighted = jnp.dot(
            jnp.concatenate(probs, axis=1), kvg[:, 128:256], preferred_element_type=F32
        )
        weighted = weighted / row_sum
        low = lax.broadcasted_iota(I32, (BLK, 128), 1) < HD
        for p, pair in enumerate(PAIRS):
            tile = jnp.where(
                low,
                weighted[pair[0] * BLK : (pair[0] + 1) * BLK],
                weighted[pair[1] * BLK : (pair[1] + 1) * BLK],
            )
            att[pl.ds(pl.multiple_of(r * BLK, BLK), BLK), 128 * p : 128 * (p + 1)] = tile.astype(
                BF16
            )
        lsum[r] = jnp.broadcast_to(row_sum, (TOK, 128))
        return carry

    def out_copy(piece):
        return remote(
            part.at[piece], part_in.at[piece], out_send.at[piece], out_recv.at[piece], partner
        )

    def do_piece(piece, carry):
        for r in range(PER):
            attend(piece * PER + r, 0)
        at = pl.ds(pl.multiple_of(piece * PER * BLK, PER * BLK), PER * BLK)
        theirs = pl.multiple_of((1 - tp) * 512, 512)
        part[piece] = jnp.dot(
            att[at, :], wo_v[:, pl.ds(theirs, 512)], preferred_element_type=F32
        ).astype(BF16)
        out_copy(piece).start()
        return carry

    lax.fori_loop(0, PIECES, do_piece, 0)
    out_copies = [out_copy(piece) for piece in range(PIECES)]
    lane_q = lax.broadcasted_iota(I32, (TOK, 128), 1)
    query = lax.broadcasted_iota(I32, (TOK, 128), 0) % BLK
    for side in range(2):
        sums = jnp.zeros((TOK, 128), F32)
        for r in range(4):
            sums = jnp.where(lane_q == r * BLK + query, lsum[4 * side + r], sums)
        ago = (lax.broadcasted_iota(I32, (HEADS, 128), 1) % BLK).astype(F32)
        logs[:, 128 * side : 128 * (side + 1)] = jnp.log(
            jnp.sum(sums.reshape(HEADS, BLK, 128), axis=1)
        ) - slope[...] * ago * (1.0 / LOG2E)
    mine = pl.multiple_of(tp * 512, 512)
    for piece in range(PIECES):
        at = pl.ds(piece * PER * BLK, PER * BLK)
        own = jnp.dot(att[at, :], wo_v[:, pl.ds(mine, 512)], preferred_element_type=F32)
        out_copies[piece].wait_recv()
        out[at, :] = (own + part_in[piece].astype(F32)).astype(BF16)

    for c in tok_copies + nsel_copies + plane_copies + out_copies + list(y_copies.values()):
        c.wait_send()
    for step in ups + downs:
        for c in step:
            c.wait_send()


def deliver(mixed, logs, mixed_out, logs_out, sem):
    copies = (
        pltpu.make_async_copy(mixed, mixed_out, sem.at[0]),
        pltpu.make_async_copy(logs, logs_out, sem.at[1]),
    )
    for c in copies:
        c.start()
    for c in copies:
        c.wait()


def body(tokens, norm_gain, w_query, w_key, w_value, q_gain, k_gain, w_out, chosen):
    hbm = pl.BlockSpec(memory_space=pltpu.HBM)
    vmem = pl.BlockSpec(memory_space=pltpu.VMEM)
    dma = pltpu.SemaphoreType.DMA
    mixed, logs = pl.pallas_call(
        kernel,
        out_shape=(
            jax.ShapeDtypeStruct((TOK, 512), BF16),
            jax.ShapeDtypeStruct((HEADS, TOK), F32),
        ),
        in_specs=[hbm] * 9,
        out_specs=(vmem, vmem),
        scratch_shapes=[
            pltpu.VMEM((NB, TOPB), I32),
            pltpu.VMEM((1, 1024), F32),
            pltpu.VMEM((1, HD), F32),
            pltpu.VMEM((1, HD), F32),
            pltpu.VMEM((2, TOK, 512), BF16),
            pltpu.VMEM((TOK, 1024), BF16),
            pltpu.VMEM((1024, 512), BF16),
            pltpu.VMEM((1024, 256), BF16),
            pltpu.VMEM((512, 1024), BF16),
            *[pltpu.VMEM((NB, BLK, 256), BF16) for _ in range(11)],
            pltpu.VMEM((NZ * NY, MOST, BLK, 256), BF16),
            pltpu.VMEM((LANDED, BLK, 256), BF16),
            pltpu.VMEM((NB, 256), I32),
            pltpu.VMEM((len(SERVED), NB, 256), I32),
            pltpu.VMEM((NB, 128), I32),
            pltpu.SMEM((NB, 256), I32),
            pltpu.SMEM((len(SERVED), NB, 256), I32),
            pltpu.SMEM((NB, 128), I32),
            pltpu.VMEM((NB, 8, TOPB * BLK), F32),
            pltpu.VMEM((HEADS, 128), F32),
            pltpu.VMEM((NB, TOK, 128), BF16),
            pltpu.VMEM((TOPB * BLK, 256), BF16),
            pltpu.VMEM((TOK, 512), BF16),
            pltpu.VMEM((NB, TOK, 128), F32),
            pltpu.VMEM((PIECES, PER * BLK, 512), BF16),
            pltpu.VMEM((PIECES, PER * BLK, 512), BF16),
            dma((4,)),
            dma((CHUNKS,)),
            dma((11,)),
            dma((2 + len(SERVED),)),
            dma((CHUNKS,)), dma((CHUNKS,)),
            dma((len(SERVED),)), dma((len(SERVED),)),
            dma((4 * CHUNKS,)), dma((4 * CHUNKS,)),
            dma((3 * CHUNKS,)), dma((3 * CHUNKS,)),
            dma((NY * CHUNKS,)), dma((NY * CHUNKS,)),
            dma((NZ * NY,)), dma((NZ * NY,)),
            dma((PIECES,)), dma((PIECES,)),
        ],
        compiler_params=pltpu.CompilerParams(
            collective_id=0, has_side_effects=True, vmem_limit_bytes=54700 * 1024
        ),
        name="fused",
    )(
        tokens.reshape(TOK, 512),
        norm_gain.reshape(1, 1024),
        w_query,
        w_key,
        w_value,
        q_gain.reshape(1, HD),
        k_gain.reshape(1, HD),
        w_out,
        chosen.reshape(NB, TOPB),
    )
    mixed, logs = pl.pallas_call(
        deliver,
        out_shape=(
            jax.ShapeDtypeStruct((TOK, 512), BF16),
            jax.ShapeDtypeStruct((HEADS, TOK), F32),
        ),
        in_specs=[vmem, vmem],
        out_specs=(hbm, hbm),
        scratch_shapes=[dma((2,))],
        compiler_params=pltpu.CompilerParams(vmem_limit_bytes=8 * 1024 * 1024),
        name="deliver",
    )(mixed, logs)
    return mixed.reshape(1, TOK, 512), logs.reshape(1, HEADS, TOK)


def solution(mesh):
    return jax.shard_map(
        body,
        mesh=mesh,
        in_specs=(
            P("dp", "kv", "tp"), P(), P(None, "tp"), P(None, "tp"), P(None, "tp"),
            P(), P(), P("tp", None), P("dp", "kv", None),
        ),
        out_specs=(P("dp", "kv", "tp"), P("dp", "tp", "kv")),
        check_vma=False,
    )
```

```python
import functools
import math

import jax
import jax.numpy as jnp
from jax import lax
from jax.experimental import pallas as pl
from jax.experimental.pallas import tpu as pltpu
from jax.sharding import PartitionSpec as P

MESH = pl.DeviceIdType.MESH
F32 = jnp.float32
BF16 = jnp.bfloat16
I32 = jnp.int32

NZ, NY = 8, 4
NB = 8
BLK = 32
TOPB = 16
MOST = 4
HD = 64
HEADS = 8
TOK = NB * BLK
EPS = 1e-6
SEQ = 8192
OWN = NZ * NY * MOST
LANDED = OWN + NB
FAR = -1e30
PAIRS = ((0, 5), (2, 7), (1, 4), (3, 6))
DIRECT = ((7, 1), (7, 2), (7, 3), (2, 2), (6, 2))
SERVED = ((0, 1), (0, 2), (0, 3)) + tuple(
    (d if d <= 4 else d - 8, 0) for d in sorted({d for d, _ in DIRECT})
)
NEAR = tuple(sorted({(1, 0), (-1, 0), *SERVED, *((-dz, -dy % 4) for dz, dy in SERVED)}))
CHUNKS = 4
STEP = TOK // CHUNKS
PIECES = 2
PER = NB // PIECES
LOG2E = math.log2(math.e)


def half_sums(x):
    row = lax.broadcasted_iota(I32, (128, 128), 0) // HD
    col = lax.broadcasted_iota(I32, (128, 128), 1) // HD
    ones = jnp.where(row == col, 1.0, 0.0).astype(BF16)
    high = x.astype(BF16)
    low = (x - high.astype(F32)).astype(BF16)
    return jnp.dot(high, ones, preferred_element_type=F32) + jnp.dot(
        low, ones, preferred_element_type=F32
    )


def head_norm(x, gain):
    return x * lax.rsqrt(half_sums(x * x) * (1.0 / HD) + EPS) * gain


def kernel(
    tokens, gain_h, wq, wk, wv, qg_h, kg_h, wo, chosen_h,
    out, logs,
    chosen, gain, qg, kg, tok, hid, wq_v, wkv_v, wo_v,
    c0, c1, c2, c3, c4, c5, c6, c7, p1, p2, p3,
    msg, land, sel_v, nsel_v, ent_v, sel_s, nsel_s, ent_s,
    upos, slope, qbd, kvg, att, lsum, part, part_in,
    small_sem, mine_sem, load_sem, tab_sem, tok_send, tok_recv, nsel_send, nsel_recv,
    up_send, up_recv, dn_send, dn_recv, pln_send, pln_recv, y_send, y_recv, out_send, out_recv,
):
    dp = lax.axis_index("dp")
    kv = lax.axis_index("kv")
    tp = lax.axis_index("tp")
    z = kv // NY
    y = kv % NY
    col = (c0, c1, c2, c3, c4, c5, c6, c7)
    plane = (c0, p1, p2, p3)

    def dev(dz, dy):
        return (dp, ((z + dz) % NZ) * NY + (y + dy) % NY, tp)

    partner = (dp, kv, 1 - tp)

    def remote(src, dst, send, recv, where):
        return pltpu.make_async_remote_copy(
            src_ref=src, dst_ref=dst, send_sem=send, recv_sem=recv,
            device_id=where, device_id_type=MESH,
        )

    barrier = pltpu.get_barrier_semaphore()
    peers = [partner] + [dev(*at) for at in NEAR]
    for peer in peers:
        pl.semaphore_signal(barrier, inc=1, device_id=peer, device_id_type=MESH)

    small = [
        pltpu.make_async_copy(src, dst, small_sem.at[n])
        for n, (src, dst) in enumerate(
            ((chosen_h, chosen), (gain_h, gain), (qg_h, qg), (kg_h, kg))
        )
    ]
    for load in small:
        load.start()
    tok_loads = [
        pltpu.make_async_copy(
            tokens.at[pl.ds(i * STEP, STEP)], tok.at[tp, pl.ds(i * STEP, STEP)], mine_sem.at[i]
        )
        for i in range(CHUNKS)
    ]
    loads = [
        pltpu.make_async_copy(wk, wkv_v.at[:, pl.ds(0, 128)], load_sem.at[0]),
        pltpu.make_async_copy(wv, wkv_v.at[:, pl.ds(128, 128)], load_sem.at[1]),
        pltpu.make_async_copy(wq, wq_v, load_sem.at[2]),
    ]
    for p, pair in enumerate(PAIRS):
        for side in range(2):
            loads.append(
                pltpu.make_async_copy(
                    wo.at[pl.ds(pair[side] * HD, HD), :],
                    wo_v.at[pl.ds(p * 128 + side * HD, HD), :],
                    load_sem.at[3 + 2 * p + side],
                )
            )
    for load in tok_loads + loads:
        load.start()

    small[0].wait()
    ch = chosen[...]
    lane = lax.broadcasted_iota(I32, (NB, 256), 1)
    own_block = kv * NB + lax.broadcasted_iota(I32, (NB, 1), 0)
    member = jnp.zeros((NB, 256), I32)
    for e in range(TOPB):
        member = jnp.where(ch[:, e : e + 1] == lane, 1, member)
    present = jnp.broadcast_to(jnp.max(member, axis=0, keepdims=True), (NB, 256))
    inner = lane % NB
    rank = jnp.zeros((NB, 256), I32)
    for k in range(1, NB):
        rank = rank + jnp.where(inner >= k, pltpu.roll(present, k, 1), 0)
    sub = lax.broadcasted_iota(I32, (NB, 256), 0)
    sel = jnp.zeros((NB, 256), I32)
    for s in range(MOST):
        val = jnp.where((present == 1) & (rank == s), inner, 0)
        for k in (1, 2, 4):
            val = val + pltpu.roll(val, 256 - k, 1)
        sel = jnp.where(sub == s, val, sel)
    sel_v[...] = sel
    chip = lane // NB
    from_y = (y - chip % NY + NY) % NY
    from_z = (z - chip // NY + NZ) % NZ
    spot_of = jnp.where(
        chip == kv,
        OWN + inner,
        (from_y * NZ + from_z) * MOST + rank,
    )
    front = jnp.where(
        lax.broadcasted_iota(I32, (NB, TOPB), 1) == 0,
        own_block,
        jnp.where(ch == own_block, ch[:, 0:1], ch),
    )
    filled = jnp.where(front < 0, own_block, front)
    lane_e = lax.broadcasted_iota(I32, (NB, 128), 1)
    entry = jnp.zeros((NB, 128), I32)
    lane_u = lax.broadcasted_iota(I32, (NB, TOPB * BLK), 1)
    pos = jnp.full((NB, TOPB * BLK), FAR, F32)
    for e in range(TOPB):
        at = jnp.sum(jnp.where(filled[:, e : e + 1] == lane, spot_of, 0), axis=1, keepdims=True)
        entry = jnp.where(lane_e == e, at, entry)
        first = front[:, e : e + 1]
        pos = jnp.where(
            (lane_u // BLK == e) & (first >= 0),
            (first * BLK + lane_u % BLK).astype(F32),
            pos,
        )
    ent_v[...] = entry
    for r in range(NB):
        upos[r] = jnp.broadcast_to(pos[r : r + 1], (8, TOPB * BLK))

    head_no = (tp * HEADS + lax.broadcasted_iota(I32, (HEADS, 128), 0) + 1).astype(F32)
    slope[...] = jnp.exp2(head_no * (-8.0 / 16.0)) * (4.0 / SEQ * LOG2E)
    pl.semaphore_wait(barrier, len(peers))
    tok_copies = []
    for i in range(CHUNKS):
        at = pl.ds(i * STEP, STEP)
        tok_loads[i].wait()
        c = remote(tok.at[tp, at], tok.at[tp, at], tok_send.at[i], tok_recv.at[i], partner)
        c.start()
        tok_copies.append(c)

    nsel_copies = []
    for n, (dz, dy) in enumerate(SERVED):
        c = remote(sel_v, nsel_v.at[n], nsel_send.at[n], nsel_recv.at[n], dev(-dz, -dy))
        c.start()
        nsel_copies.append(c)
    tabs = [
        pltpu.make_async_copy(sel_v, sel_s, tab_sem.at[0]),
        pltpu.make_async_copy(ent_v, ent_s, tab_sem.at[1]),
    ]
    for t in tabs:
        t.start()

    for load in small[1:]:
        load.wait()
    size = NB // CHUNKS

    def up(d, part):
        at = pl.ds(part * size, size)
        n = CHUNKS * d + part
        return remote(
            col[d].at[at], col[d + 1].at[at], up_send.at[n], up_recv.at[n], dev(1, 0)
        )

    def down(d, part):
        at = pl.ds(part * size, size)
        n = CHUNKS * d + part
        return remote(
            col[(8 - d) % 8].at[at], col[7 - d].at[at], dn_send.at[n], dn_recv.at[n], dev(-1, 0)
        )

    ups = [[up(d, bit) for bit in range(CHUNKS)] for d in range(4)]
    downs = [[down(d, bit) for bit in range(CHUNKS)] for d in range(3)]
    g0 = gain[:, 0:512]
    g1 = gain[:, 512:1024]
    kgain = jnp.concatenate([kg[...], kg[...]], axis=1)
    qgain = jnp.concatenate([qg[...], qg[...]], axis=1)
    loads[0].wait()
    loads[1].wait()
    plane_copies = []
    for i in range(CHUNKS):
        tok_copies[i].wait_recv()
        for half in range(2):
            at = pl.ds(i * STEP + half * (STEP // 2), STEP // 2)
            a = tok[0, at, :].astype(F32)
            b = tok[1, at, :].astype(F32)
            total = jnp.sum(a * a + b * b, axis=1, keepdims=True)
            r = lax.rsqrt(total * (1.0 / 1024.0) + EPS)
            hid[at, 0:512] = (a * r * g0).astype(BF16)
            hid[at, 512:1024] = (b * r * g1).astype(BF16)
        both = jnp.dot(hid[pl.ds(i * STEP, STEP), :], wkv_v[...], preferred_element_type=F32)
        keys = head_norm(both[:, 0:128], kgain).astype(BF16)
        values = both[:, 128:256].astype(BF16)
        for k, rows_of in enumerate((keys, values)):
            blocks = rows_of.reshape(size, BLK, 128)
            c0[pl.ds(i * size, size), :, 128 * k : 128 * (k + 1)] = blocks
            land[pl.ds(OWN + i * size, size), :, 128 * k : 128 * (k + 1)] = blocks
        ups[0][i].start()
        downs[0][i].start()
        for dy in (1, 3, 2):
            at = pl.ds(i * size, size)
            n = dy * CHUNKS + i
            c = remote(c0.at[at], plane[dy].at[at], pln_send.at[n], pln_recv.at[n], dev(0, dy))
            c.start()
            plane_copies.append(c)

    y_copies = {}

    def picked(table, source, d, dy, s):
        which = table[s, source * NB]
        return plane[dy][which] if d == 0 else col[d][which]

    def device_no(dz, dy):
        return ((z + dz + NZ) % NZ) * NY + (y + dy + NY) % NY

    def send(n, k, source, d, dy):
        slot = k % NZ
        c = remote(
            msg.at[k], land.at[pl.ds(k * MOST, MOST)],
            y_send.at[k], y_recv.at[k], dev(*SERVED[n]),
        )
        wanted = (z + SERVED[n][0] + NZ) % NZ >= slot
        y_copies[k] = (c, wanted, z >= slot)

        @pl.when(wanted)
        def _():
            for s in range(MOST):
                msg[k, s] = picked(nsel_s.at[n], source, d, dy, s)
            c.start()

    def serve(d):
        for n, dy in ((0, 1), (2, 3), (1, 2)):
            if (d, dy) not in DIRECT:
                send(n, dy * NZ + d, device_no(-d, 0), d, 0)

    def keep(d, dy):
        for s in range(MOST):
            land[(dy * NZ + d) * MOST + s] = picked(sel_s, device_no(-d, -dy), d, dy, s)

    def turn(k):
        for bit in range(CHUNKS):
            ups[k - 1][bit].wait_recv()
            if k < 4:
                ups[k][bit].start()
                downs[k - 1][bit].wait_recv()
            if k < 3:
                downs[k][bit].start()

    for c in nsel_copies:
        c.wait_recv()
    ntab = [
        pltpu.make_async_copy(nsel_v.at[n], nsel_s.at[n], tab_sem.at[2 + n])
        for n in range(len(SERVED))
    ]
    for t in ntab:
        t.start()
    for t in tabs + ntab:
        t.wait()

    low_half = lax.broadcasted_iota(I32, (TOK, 128), 1) < HD

    def queries(one, two, pair, turned):
        flat = [
            jnp.dot(hid[...], wq_v[:, 128 * t : 128 * (t + 1)], preferred_element_type=F32)
            for t in (one, two)
        ]
        a, b = (head_norm(x, qgain) for x in flat)
        for (lo, hi), roll in ((pair, False), (turned, True)):
            if roll:
                a, b = pltpu.roll(a, HD, 1), pltpu.roll(b, HD, 1)
            first = jnp.where(low_half, a, 0.0).astype(BF16)
            second = jnp.where(low_half, 0.0, b).astype(BF16)
            for r in range(NB):
                qbd[r, pl.ds(lo * BLK, BLK), :] = first[r * BLK : (r + 1) * BLK]
                qbd[r, pl.ds(hi * BLK, BLK), :] = second[r * BLK : (r + 1) * BLK]

    turn(1)
    serve(1)
    keep(1, 0)
    keep(7, 0)
    loads[2].wait()
    queries(0, 2, PAIRS[0], PAIRS[2])
    turn(2)
    serve(2)
    serve(6)
    for c in plane_copies:
        c.wait_recv()
    for d, dy in DIRECT:
        to = SERVED.index((d if d <= 4 else d - 8, 0))
        send(to, dy * NZ + d, device_no(0, -dy), 0, dy)
    for dy in (1, 2, 3):
        keep(0, dy)
    keep(2, 0)
    keep(6, 0)
    queries(1, 3, PAIRS[1], PAIRS[3])
    turn(3)
    serve(3)
    serve(5)
    keep(3, 0)
    keep(5, 0)
    turn(4)
    serve(4)
    keep(4, 0)
    for load in loads[3:]:
        load.wait()
    for c, _, awaited in y_copies.values():
        pl.when(awaited)(c.wait_recv)

    def attend(r, carry):
        for e in range(TOPB):
            kvg[pl.ds(e * BLK, BLK), :] = land[ent_s[r, e]]
        raw = lax.dot_general(
            qbd[r], kvg[:, 0:128], (((1,), (1,)), ((), ())), preferred_element_type=F32
        )
        total = jnp.zeros((TOK, 128), F32)
        probs = []
        first_key = (kv * NB + r) * BLK
        later = lax.broadcasted_iota(I32, (BLK, 128), 1) > lax.broadcasted_iota(
            I32, (BLK, 128), 0
        )
        own_lane = lax.broadcasted_iota(I32, (BLK, 128), 1) < BLK
        for i in range(4):
            off = upos[r, :, 128 * i : 128 * (i + 1)] - first_key.astype(F32)
            factor = jnp.exp2(slope[...] * off)
            w = jnp.exp2(raw[:, 128 * i : 128 * (i + 1)] * (LOG2E / 8.0)).reshape(
                HEADS, BLK, 128
            ) * factor.reshape(HEADS, 1, 128)
            if i == 0:
                w = jnp.where((later & own_lane)[None], 0.0, w)
            w = w.reshape(TOK, 128)
            total = total + w
            probs.append(w.astype(BF16))
        row_sum = jnp.sum(total, axis=1, keepdims=True)
        weighted = jnp.dot(
            jnp.concatenate(probs, axis=1), kvg[:, 128:256], preferred_element_type=F32
        )
        weighted = weighted / row_sum
        low = lax.broadcasted_iota(I32, (BLK, 128), 1) < HD
        for p, pair in enumerate(PAIRS):
            tile = jnp.where(
                low,
                weighted[pair[0] * BLK : (pair[0] + 1) * BLK],
                weighted[pair[1] * BLK : (pair[1] + 1) * BLK],
            )
            att[pl.ds(pl.multiple_of(r * BLK, BLK), BLK), 128 * p : 128 * (p + 1)] = tile.astype(
                BF16
            )
        lsum[r] = jnp.broadcast_to(row_sum, (TOK, 128))
        return carry

    def out_copy(piece):
        return remote(
            part.at[piece], part_in.at[piece], out_send.at[piece], out_recv.at[piece], partner
        )

    def do_piece(piece, carry):
        for r in range(PER):
            attend(piece * PER + r, 0)
        at = pl.ds(pl.multiple_of(piece * PER * BLK, PER * BLK), PER * BLK)
        theirs = pl.multiple_of((1 - tp) * 512, 512)
        part[piece] = jnp.dot(
            att[at, :], wo_v[:, pl.ds(theirs, 512)], preferred_element_type=F32
        ).astype(BF16)
        out_copy(piece).start()
        return carry

    lax.fori_loop(0, PIECES, do_piece, 0)
    out_copies = [out_copy(piece) for piece in range(PIECES)]
    for c in tok_copies + nsel_copies + plane_copies:
        c.wait_send()
    for c, wanted, _ in y_copies.values():
        pl.when(wanted)(c.wait_send)
    for step in ups + downs:
        for c in step:
            c.wait_send()

    lane_q = lax.broadcasted_iota(I32, (TOK, 128), 1)
    query = lax.broadcasted_iota(I32, (TOK, 128), 0) % BLK
    for side in range(2):
        sums = jnp.zeros((TOK, 128), F32)
        for r in range(4):
            sums = jnp.where(lane_q == r * BLK + query, lsum[4 * side + r], sums)
        ago = (lax.broadcasted_iota(I32, (HEADS, 128), 1) % BLK).astype(F32)
        logs[:, 128 * side : 128 * (side + 1)] = jnp.log(
            jnp.sum(sums.reshape(HEADS, BLK, 128), axis=1)
        ) - slope[...] * ago * (1.0 / LOG2E)
    mine = pl.multiple_of(tp * 512, 512)
    for piece in range(PIECES):
        at = pl.ds(piece * PER * BLK, PER * BLK)
        own = jnp.dot(att[at, :], wo_v[:, pl.ds(mine, 512)], preferred_element_type=F32)
        out_copies[piece].wait_recv()
        out[at, :] = (own + part_in[piece].astype(F32)).astype(BF16)
    for c in out_copies:
        c.wait_send()


def deliver(mixed, logs, mixed_out, logs_out, sem):
    copies = (
        pltpu.make_async_copy(mixed, mixed_out, sem.at[0]),
        pltpu.make_async_copy(logs, logs_out, sem.at[1]),
    )
    for c in copies:
        c.start()
    for c in copies:
        c.wait()


def body(tokens, norm_gain, w_query, w_key, w_value, q_gain, k_gain, w_out, chosen):
    hbm = pl.BlockSpec(memory_space=pltpu.HBM)
    vmem = pl.BlockSpec(memory_space=pltpu.VMEM)
    dma = pltpu.SemaphoreType.DMA
    mixed, logs = pl.pallas_call(
        kernel,
        out_shape=(
            jax.ShapeDtypeStruct((TOK, 512), BF16),
            jax.ShapeDtypeStruct((HEADS, TOK), F32),
        ),
        in_specs=[hbm] * 9,
        out_specs=(vmem, vmem),
        scratch_shapes=[
            pltpu.VMEM((NB, TOPB), I32),
            pltpu.VMEM((1, 1024), F32),
            pltpu.VMEM((1, HD), F32),
            pltpu.VMEM((1, HD), F32),
            pltpu.VMEM((2, TOK, 512), BF16),
            pltpu.VMEM((TOK, 1024), BF16),
            pltpu.VMEM((1024, 512), BF16),
            pltpu.VMEM((1024, 256), BF16),
            pltpu.VMEM((512, 1024), BF16),
            *[pltpu.VMEM((NB, BLK, 256), BF16) for _ in range(11)],
            pltpu.VMEM((NZ * NY, MOST, BLK, 256), BF16),
            pltpu.VMEM((LANDED, BLK, 256), BF16),
            pltpu.VMEM((NB, 256), I32),
            pltpu.VMEM((len(SERVED), NB, 256), I32),
            pltpu.VMEM((NB, 128), I32),
            pltpu.SMEM((NB, 256), I32),
            pltpu.SMEM((len(SERVED), NB, 256), I32),
            pltpu.SMEM((NB, 128), I32),
            pltpu.VMEM((NB, 8, TOPB * BLK), F32),
            pltpu.VMEM((HEADS, 128), F32),
            pltpu.VMEM((NB, TOK, 128), BF16),
            pltpu.VMEM((TOPB * BLK, 256), BF16),
            pltpu.VMEM((TOK, 512), BF16),
            pltpu.VMEM((NB, TOK, 128), F32),
            pltpu.VMEM((PIECES, PER * BLK, 512), BF16),
            pltpu.VMEM((PIECES, PER * BLK, 512), BF16),
            dma((4,)),
            dma((CHUNKS,)),
            dma((11,)),
            dma((2 + len(SERVED),)),
            dma((CHUNKS,)), dma((CHUNKS,)),
            dma((len(SERVED),)), dma((len(SERVED),)),
            dma((4 * CHUNKS,)), dma((4 * CHUNKS,)),
            dma((3 * CHUNKS,)), dma((3 * CHUNKS,)),
            dma((NY * CHUNKS,)), dma((NY * CHUNKS,)),
            dma((NZ * NY,)), dma((NZ * NY,)),
            dma((PIECES,)), dma((PIECES,)),
        ],
        compiler_params=pltpu.CompilerParams(
            collective_id=0, has_side_effects=True, vmem_limit_bytes=54700 * 1024
        ),
        name="fused",
    )(
        tokens.reshape(TOK, 512),
        norm_gain.reshape(1, 1024),
        w_query,
        w_key,
        w_value,
        q_gain.reshape(1, HD),
        k_gain.reshape(1, HD),
        w_out,
        chosen.reshape(NB, TOPB),
    )
    mixed, logs = pl.pallas_call(
        deliver,
        out_shape=(
            jax.ShapeDtypeStruct((TOK, 512), BF16),
            jax.ShapeDtypeStruct((HEADS, TOK), F32),
        ),
        in_specs=[vmem, vmem],
        out_specs=(hbm, hbm),
        scratch_shapes=[dma((2,))],
        compiler_params=pltpu.CompilerParams(vmem_limit_bytes=8 * 1024 * 1024),
        name="deliver",
    )(mixed, logs)
    return mixed.reshape(1, TOK, 512), logs.reshape(1, HEADS, TOK)


def solution(mesh):
    return jax.shard_map(
        body,
        mesh=mesh,
        in_specs=(
            P("dp", "kv", "tp"), P(), P(None, "tp"), P(None, "tp"), P(None, "tp"),
            P(), P(), P("tp", None), P("dp", "kv", None),
        ),
        out_specs=(P("dp", "kv", "tp"), P("dp", "tp", "kv")),
        check_vma=False,
    )
```
